256 devices in a mesh: sp: 32 (over z, y), tp: 8 (over x, core).
Axes of the slice: x: 4, y: 4, z: 8, core: 2. Of those that a mesh axis runs over, the one named last changes fastest.
Arguments:
- queries: bfloat16 [32768, 1024], P('sp', 'tp'), may hold values from -6 to 6
- cell_key_rows: bfloat16 [32768, 1024], P('sp', 'tp'), may hold values from -6 to 6
- cell_value_rows: bfloat16 [32768, 2048], P('sp', 'tp'), may hold values from -6 to 6
- output_gate_logits: bfloat16 [32768, 2048], P('sp', 'tp'), may hold values from -6 to 6
- input_gate_logits: bfloat16 [8, 32768], P('tp', 'sp'), may hold values from -4 to 216
- forget_gate_logits: bfloat16 [8, 32768], P('tp', 'sp'), may hold values from 0.5 to 14
- forget_extra_term: float32 [8, 32768], P('tp', 'sp'), may hold values from -1.4 to 0
- residual: bfloat16 [32768, 2048], P('sp', 'tp'), may hold values from -13 to 13
- head_norm_gain: bfloat16 [2048], P('tp'), may hold values from 0.099609375 to 1.8984375
- cell_output_weight: bfloat16 [2048, 2048], P('tp'), may hold values from -0.25 to 0.25
- feedforward_norm_gain: bfloat16 [2048], replicated, may hold values from 0.099609375 to 1.8984375
- gate_projection_weight: bfloat16 [2048, 5632], P('sp', 'tp'), may hold values from -0.125 to 0.125
- up_projection_weight: bfloat16 [2048, 5632], P('sp', 'tp'), may hold values from -0.125 to 0.125
- down_projection_weight: bfloat16 [5632, 2048], P('tp', 'sp'), may hold values from -0.15625 to 0.15625
Outputs:
- mixed: bfloat16 [32768, 2048], P('sp', 'tp')
The draws below stay inside these ranges and needn't reach their ends.
All inputs are finite; a program needn't handle non-finite values.
Results may differ from the reference program's by a relative error of at most 0.017.
Values may be sent and summed in bfloat16 or wider, within the bound.
A program may use at most 64 MiB of HBM per device.

```python
import jax
import jax.numpy as jnp
from jax import lax

D = 2048
HEADS = 8
DK = 128
DV = 256
FF = 5632
TOK_DEV = 1024
TOKENS = 32768
N_TP = 8


def draw_input_gate_logits(key, part):
    base_key = jax.random.fold_in(key, 11)
    values = jnp.clip(jax.random.normal(base_key, (HEADS, TOKENS), jnp.float32), -4.0, 4.0)
    return values.astype(jnp.bfloat16)


def draw_forget_gate_logits(key, part):
    order = jax.random.permutation(jax.random.fold_in(key, 21), HEADS)
    noise_key = jax.random.fold_in(key, 22)
    slow_count = HEADS // 2
    jitter = 0.6 * jnp.clip(jax.random.normal(noise_key, (HEADS, TOKENS), jnp.float32), -4.0, 4.0)
    slow_heads = order < slow_count
    quick = jnp.log(jax.random.uniform(jax.random.fold_in(key, 23), (HEADS,), jnp.float32, 30.0, 60.0))
    level = jnp.where(slow_heads, jnp.log(TOKENS / 0.8), quick)
    block_shift = jax.random.uniform(jax.random.fold_in(key, 24), (HEADS, TOKENS // TOK_DEV), jnp.float32, -0.4, 0.4)
    shifts = jnp.repeat(block_shift, TOK_DEV, axis=1)
    return (level[:, None] + shifts + jitter).astype(jnp.bfloat16)


def draw_forget_extra_term(key, part):
    spots = jax.random.randint(jax.random.fold_in(key, 31), (HEADS, 2, 1), 0, TOKENS)
    fraction = jax.random.uniform(jax.random.fold_in(key, 32), (HEADS, 2, 1), jnp.float32, 0.2, 0.5)
    depth = jnp.log(1.0 - fraction)
    places = jnp.arange(TOKENS)[None, None, :]
    return jnp.sum(jnp.where(places == spots, depth, 0.0), axis=1).astype(jnp.float32)


def draw_residual(key, part):
    column_scale = 0.4 * 6.0 ** (jnp.arange(D, dtype=jnp.float32) / D)
    values = jnp.clip(jax.random.normal(jax.random.fold_in(key, 41), (TOKENS, D), jnp.float32), -4.0, 4.0)
    return (values * column_scale[None, :]).astype(jnp.bfloat16)


def block_levels(rng, dims, shards, low, largest):
    factor_of, own = 1.0, jax.random.fold_in(rng, 6)
    for position, parts in shards:
        steps = jnp.exp(jax.random.uniform(jax.random.fold_in(own, position), (parts,), jnp.float32, low / len(shards), largest / len(shards)))
        factor_of = factor_of * jnp.repeat(steps, dims[position] // parts).reshape([-1 if axis == position else 1 for axis in range(len(dims))])
    return factor_of


def normal_values(rng, shape, spread, most, split=(), held_as=jnp.bfloat16):
    loudness = block_levels(rng, shape, split, -0.22, 0.18) if split else 1.0
    result = jax.random.normal(rng, shape, jnp.float32) * spread * loudness
    return jnp.minimum(jnp.maximum(result, -most), most).astype(held_as)


def setup_inputs(seed: int = 0) -> dict:
    arg_keys = jax.random.split(jax.random.key(seed), 15)
    return {
        "queries": normal_values(arg_keys[0], (TOKENS, HEADS * DK), 1.0, 6.0, ((0, 32), (1, 8))),
        "cell_key_rows": normal_values(arg_keys[1], (TOKENS, HEADS * DK), 1.0, 6.0, ((0, 32), (1, 8))),
        "cell_value_rows": normal_values(arg_keys[2], (TOKENS, HEADS * DV), 1.0, 6.0, ((0, 32), (1, 8))),
        "output_gate_logits": normal_values(arg_keys[3], (TOKENS, HEADS * DV), 1.0, 6.0, ((0, 32), (1, 8))),
        "input_gate_logits": draw_input_gate_logits(jax.random.fold_in(arg_keys[14], 71), 0),
        "forget_gate_logits": draw_forget_gate_logits(jax.random.fold_in(arg_keys[14], 71), 0),
        "forget_extra_term": draw_forget_extra_term(jax.random.fold_in(arg_keys[14], 71), 0),
        "residual": draw_residual(jax.random.fold_in(arg_keys[14], 71), 0),
        "head_norm_gain": jnp.clip(1.0 + 0.18 * jax.random.normal(arg_keys[8], (HEADS * DV,), jnp.float32), 0.099609375, 1.8984375).astype(jnp.bfloat16),
        "cell_output_weight": normal_values(arg_keys[9], (HEADS * DV, D), (HEADS * DV // 4) ** -0.5, 0.25, ((0, 8),)),
        "feedforward_norm_gain": jnp.clip(1.0 + 0.18 * jax.random.normal(arg_keys[10], (D,), jnp.float32), 0.099609375, 1.8984375).astype(jnp.bfloat16),
        "gate_projection_weight": normal_values(arg_keys[11], (D, FF), D ** -0.5, 0.125, ((0, 32), (1, 8))),
        "up_projection_weight": normal_values(arg_keys[12], (D, FF), D ** -0.5, 0.125, ((0, 32), (1, 8))),
        "down_projection_weight": normal_values(arg_keys[13], (FF, D), (FF // 4) ** -0.5, 0.15625, ((0, 8), (1, 32))),
    }


PRECISE = lax.Precision.HIGHEST
LOWEST_LOG = -1e+30
EPSILON = 1e-06

def to_blocks(array, block_count, block_size):
    shaped = array.reshape((array.shape[0], block_count, block_size) + array.shape[2:])
    return jnp.moveaxis(shaped, 1, 0)

def from_blocks(array):
    moved = jnp.moveaxis(array, 0, 1)
    return moved.reshape((moved.shape[0], moved.shape[1] * moved.shape[2]) + moved.shape[3:])

def memory_blocks(query_heads, key_heads, value_heads, in_gates, forget_log_value, block_size):
    head_count, length, key_width = query_heads.shape
    value_width = value_heads.shape[2]
    block_count = length // block_size
    causal = jnp.tril(jnp.ones((block_size, block_size), bool))

    def advance(carried, pieces):
        memory_state, top_log, offset = carried
        query_block, key_block, value_block, gate_block, forget_block = pieces
        running = jnp.cumsum(forget_block, axis=-1)
        log_weight = jnp.where(causal, running[:, :, None] - running[:, None, :] + gate_block[:, None, :], -jnp.inf)
        log_start = running + top_log[:, None]
        row_max = jnp.maximum(lax.optimization_barrier(jnp.max(log_weight, axis=-1)), log_start)
        scores = jnp.einsum('htd,hsd->hts', query_block, key_block, precision=PRECISE)
        scores = scores * jnp.exp(log_weight - row_max[:, :, None])
        earlier = jnp.einsum('htd,hde->hte', query_block, memory_state, precision=PRECISE)
        numerator = jnp.exp(log_start - row_max)[:, :, None] * earlier
        numerator = numerator + jnp.einsum('hts,hse->hte', scores, value_block, precision=PRECISE)
        last_cum = running[:, -1]
        log_end = last_cum[:, None] - running + gate_block
        new_top = jnp.maximum(last_cum + top_log, lax.optimization_barrier(jnp.max(log_end, axis=-1)))
        scaled = key_block * jnp.exp(log_end - new_top[:, None])[:, :, None]
        memory_state = jnp.exp(last_cum + top_log - new_top)[:, None, None] * memory_state
        memory_state = memory_state + jnp.einsum('hsd,hse->hde', scaled, value_block, precision=PRECISE)
        return ((memory_state, new_top, offset + last_cum), (numerator, row_max, offset[:, None] + running))
    initial = (jnp.zeros((head_count, key_width, value_width), jnp.float32), jnp.full((head_count,), LOWEST_LOG, jnp.float32), jnp.zeros((head_count,), jnp.float32))
    pieces = tuple((to_blocks(array, block_count, block_size) for array in (query_heads, key_heads, value_heads, in_gates, forget_log_value)))
    ending, outputs = lax.scan(advance, initial, pieces)
    return (tuple((from_blocks(output) for output in outputs)), ending)

def reference(queries, cell_key_rows, cell_value_rows, output_gate_logits, input_gate_logits, forget_gate_logits, forget_extra_term, residual, head_norm_gain, cell_output_weight, feedforward_norm_gain, gate_projection_weight, up_projection_weight, down_projection_weight):
    length = queries.shape[0]

    def heads_first(array, width):
        return jnp.transpose(array.reshape(length, HEADS, width), (1, 0, 2)).astype(jnp.float32)
    query_heads = heads_first(queries, DK) * DK ** (-0.5)
    key_heads = heads_first(cell_key_rows, DK)
    value_heads = heads_first(cell_value_rows, DV)
    forget_log_value = jax.nn.log_sigmoid(forget_gate_logits.astype(jnp.float32)) + forget_extra_term
    results, _ = memory_blocks(query_heads, key_heads, value_heads, input_gate_logits.astype(jnp.float32), forget_log_value, min(length, 256))
    memory = jnp.transpose(results[0], (1, 0, 2))
    normal = memory * lax.rsqrt(lax.optimization_barrier(jnp.mean(memory * memory, axis=-1, keepdims=True)) + EPSILON)
    gate_open = jax.nn.sigmoid(output_gate_logits.astype(jnp.float32).reshape(length, HEADS, DV))
    gated_heads = normal * head_norm_gain.astype(jnp.float32).reshape(HEADS, DV) * gate_open
    gated_heads = gated_heads.reshape(length, HEADS * DV).astype(jnp.bfloat16)
    head_width = HEADS * DV // N_TP
    stream_sum = residual.astype(jnp.float32)
    for head_part in range(N_TP):
        head_lower = head_part * head_width
        head_term = jnp.dot(gated_heads[:, head_lower:head_lower + head_width], cell_output_weight[head_lower:head_lower + head_width], preferred_element_type=jnp.float32)
        head_rounded = lax.optimization_barrier(head_term.astype(jnp.bfloat16))
        stream_sum = stream_sum + head_rounded.astype(jnp.float32)
    stream = stream_sum.astype(jnp.bfloat16)
    stream_wide = stream.astype(jnp.float32)
    scale = lax.rsqrt(lax.optimization_barrier(jnp.mean(stream_wide * stream_wide, axis=-1, keepdims=True)) + EPSILON)
    normed = (stream_wide * scale * feedforward_norm_gain.astype(jnp.float32)).astype(jnp.bfloat16)
    gate_value = jnp.dot(normed, gate_projection_weight, preferred_element_type=jnp.float32)
    lifted = jnp.dot(normed, up_projection_weight, preferred_element_type=jnp.float32)
    hidden = (jax.nn.silu(gate_value) * lifted).astype(jnp.bfloat16)
    part_width = FF // N_TP
    summed = jnp.zeros(stream_wide.shape, jnp.float32)
    for part_index in range(N_TP):
        lower = part_index * part_width
        partial_value = jnp.dot(hidden[:, lower:lower + part_width], down_projection_weight[lower:lower + part_width], preferred_element_type=jnp.float32)
        rounded = lax.optimization_barrier(partial_value.astype(jnp.bfloat16))
        summed = summed + rounded.astype(jnp.float32)
    return (stream_wide + 0.5 * summed).astype(jnp.bfloat16)
```

```python
import jax
import jax.numpy as jnp
from jax import lax
from jax.experimental import pallas as pl
from jax.experimental.pallas import tpu as pltpu
from jax.sharding import Mesh
from jax.sharding import PartitionSpec as P

MESH = pl.DeviceIdType.MESH
F32 = jnp.float32
BF16 = jnp.bfloat16
LOWEST_LOG = -1e30
EPSILON = 1e-06
NZ, NY, NX = 8, 4, 4
CHUNKS = 4


class Slots:
    def __init__(self):
        self.used = 0

    def take(self, count=1):
        first = self.used
        self.used += count
        return first


def running_rows(row, combine, identity):
    length = row.shape[1]
    lane = lax.broadcasted_iota(jnp.int32, row.shape, 1)
    step = 1
    while step < length:
        moved = jnp.where(lane >= step, pltpu.roll(row, step, 1), identity)
        row = combine(row, moved)
        step *= 2
    return row


def as_columns(row):
    return jnp.broadcast_to(row, (128, row.shape[1])).T


def wide(tile, copies):
    return jnp.concatenate([tile] * copies, axis=1)


def join(early, late):
    state_early, top_early, total_early = early
    state_late, top_late, total_late = late
    moved = top_early + total_late
    top = jnp.maximum(moved, top_late)
    left = wide(jnp.exp(moved - top)[0:1], 2)
    right = wide(jnp.exp(top_late - top)[0:1], 2)
    return (left * state_early + right * state_late, top, total_early + total_late)


def load_triple(ref, index):
    part = ref[index]
    return (part[0:32], part[32:40, 0:128], part[32:40, 128:256])


def store_triple(ref, index, triple):
    state, top, total = triple
    ref[index, 0:32, :] = state
    ref[index, 32:40, 0:128] = top
    ref[index, 32:40, 128:256] = total


def cell_kernel(
    q_ref, k_ref, v_ref, og_ref, ig_ref, fg_ref, ex_ref, res_ref, hg_ref, wo_ref, ng_ref,
    gu_in, dn_in,
    out_ref,
    gu_all, dn_all, s1_src, s1_buf, s2_src, s2_buf, s3_src, s3_buf, state_ref,
    num_ref, pbuf, prcv, qbuf, rly, rsum, fin, sbuf, nbuf, hbuf,
    ssem, rsem,
):
    z, y, x, c = (lax.axis_index(a) for a in ("z", "y", "x", "c"))
    rows = q_ref.shape[0]
    chunk = rows // CHUNKS
    half = chunk // 2
    other = 1 - c
    x_at = [lax.rem(x + d, NX) for d in range(NX)]
    y_at = [lax.rem(y + d, NY) for d in range(NY)]
    z_at = [lax.rem(z + d, NZ) for d in range(NZ)]
    to_right, to_left, to_mate = {"x": x_at[1]}, {"x": x_at[3]}, {"c": other}
    y_right, y_left = {"y": y_at[1]}, {"y": y_at[3]}
    z_right, z_left = {"z": z_at[1]}, {"z": z_at[7]}
    sends, slots = [], Slots()

    def send(src, dst, number, device):
        copy = pltpu.make_async_remote_copy(
            src_ref=src, dst_ref=dst, send_sem=ssem.at[number], recv_sem=rsem.at[number],
            device_id=device, device_id_type=MESH,
        )
        copy.start()
        sends.append(copy)

    def arrived(dst, number):
        pltpu.make_async_remote_copy(
            src_ref=dst, dst_ref=dst, send_sem=ssem.at[number], recv_sem=rsem.at[number],
            device_id=to_mate, device_id_type=MESH,
        ).wait_recv()

    for j in range(NZ):
        store_triple(
            s2_buf, j,
            (jnp.zeros((32, 256), F32), jnp.full((8, 128), LOWEST_LOG, F32), jnp.zeros((8, 128), F32)),
        )
    gu_all[z * NY + y] = gu_in[...]
    dn_all[z * NY + y] = dn_in[...]

    barrier = pltpu.get_barrier_semaphore()
    partners = [to_right, to_left, to_mate]
    partners += [{"y": y_at[d]} for d in range(1, NY)] + [{"z": z_at[d]} for d in range(1, NZ)]
    for device in partners:
        pl.semaphore_signal(barrier, inc=1, device_id=device, device_id_type=MESH)
    pl.semaphore_wait(barrier, len(partners))

    gz_r, gz_l = slots.take(4), slots.take(4)
    gy_r, gy_l, gy_fr, gy_fl = slots.take(8), slots.take(8), slots.take(8), slots.take(8)
    dy = slots.take(4)
    dz_r, dz_l = slots.take(4), slots.take(4)
    z_order = [0, 7, 1, 6, 2, 5, 3, 4]
    piece = gu_in.shape[0] // 2

    def gu_z_send(step):
        if step == 0:
            at = gu_all.at[z * NY + y]
            send(gu_in, at, gz_r, z_right)
            send(gu_in, at, gz_l, z_left)
        elif step < 3:
            for number, d, device in ((gz_r, NZ - step, z_right), (gz_l, step, z_left)):
                at = gu_all.at[z_at[d] * NY + y]
                send(at, at, number + step, device)
        else:
            at = gu_all.at[z_at[5] * NY + y, pl.ds(0, piece)]
            send(at, at, gz_r + 3, z_right)
            at = gu_all.at[z_at[3] * NY + y, pl.ds(piece, piece)]
            send(at, at, gz_l + 3, z_left)

    def gu_z_wait(step):
        if step < 3:
            arrived(gu_all.at[z_at[7 - step] * NY + y], gz_r + step)
            arrived(gu_all.at[z_at[1 + step] * NY + y], gz_l + step)
        else:
            arrived(gu_all.at[z_at[4] * NY + y, pl.ds(0, piece)], gz_r + 3)
            arrived(gu_all.at[z_at[4] * NY + y, pl.ds(piece, piece)], gz_l + 3)

    def gu_y_send(k):
        at = gu_all.at[z_at[z_order[k]] * NY + y]
        src = gu_in if k == 0 else at
        send(src, at, gy_r + k, y_right)
        send(src, at, gy_l + k, y_left)

    def gu_y_forward(k):
        block = z_at[z_order[k]] * NY
        arrived(gu_all.at[block + y_at[3]], gy_r + k)
        at = gu_all.at[block + y_at[3], pl.ds(0, piece)]
        send(at, at, gy_fr + k, y_right)
        arrived(gu_all.at[block + y_at[1]], gy_l + k)
        at = gu_all.at[block + y_at[1], pl.ds(piece, piece)]
        send(at, at, gy_fl + k, y_left)

    def gu_y_wait(k):
        block = z_at[z_order[k]] * NY
        arrived(gu_all.at[block + y_at[2], pl.ds(0, piece)], gy_fr + k)
        arrived(gu_all.at[block + y_at[2], pl.ds(piece, piece)], gy_fl + k)

    def dn_y_send():
        at = dn_all.at[z * NY + y]
        send(dn_in, at, dy, y_right)
        send(dn_in, at, dy + 1, y_left)

    def dn_y_forward():
        arrived(dn_all.at[z * NY + y_at[3]], dy)
        at = dn_all.at[z * NY + y_at[3], pl.ds(0, piece)]
        send(at, at, dy + 2, y_right)
        arrived(dn_all.at[z * NY + y_at[1]], dy + 1)
        at = dn_all.at[z * NY + y_at[1], pl.ds(piece, piece)]
        send(at, at, dy + 3, y_left)

    def dn_y_wait():
        arrived(dn_all.at[z * NY + y_at[2], pl.ds(0, piece)], dy + 2)
        arrived(dn_all.at[z * NY + y_at[2], pl.ds(piece, piece)], dy + 3)

    def dn_z_send(step):
        if step < 3:
            for number, d, device in ((dz_r, (NZ - step) % NZ, z_right), (dz_l, step, z_left)):
                at = dn_all.at[pl.ds(z_at[d] * NY, NY)]
                send(at, at, number + step, device)
        else:
            at = dn_all.at[pl.ds(z_at[5] * NY, 2)]
            send(at, at, dz_r + 3, z_right)
            at = dn_all.at[pl.ds(z_at[3] * NY + 2, 2)]
            send(at, at, dz_l + 3, z_left)

    def dn_z_wait(step):
        if step < 3:
            arrived(dn_all.at[pl.ds(z_at[7 - step] * NY, NY)], dz_r + step)
            arrived(dn_all.at[pl.ds(z_at[1 + step] * NY, NY)], dz_l + step)
        else:
            arrived(dn_all.at[pl.ds(z_at[4] * NY, 2)], dz_r + 3)
            arrived(dn_all.at[pl.ds(z_at[4] * NY + 2, 2)], dz_l + 3)

    gu_z_send(0)
    dn_y_send()

    logits = fg_ref[...].astype(F32)
    log_forget = jnp.minimum(logits, 0.0) - jnp.log1p(jnp.exp(-jnp.abs(logits))) + ex_ref[...]
    cum = running_rows(log_forget, jnp.add, 0.0)
    lead = ig_ref[...].astype(F32) - cum
    top_run = running_rows(lead, jnp.maximum, -jnp.inf)
    last_cum = cum[:, rows - 1 :]
    last_lead = top_run[:, rows - 1 :]
    weight = as_columns(jnp.exp(lead - last_lead))
    scaled = (k_ref[...].astype(F32) * weight).astype(BF16)
    end_state = lax.dot_general(
        scaled, v_ref[...], (((0,), (0,)), ((), ())), preferred_element_type=F32
    )
    end_top = jnp.broadcast_to(last_cum + last_lead, (8, 128))
    end_total = jnp.broadcast_to(last_cum, (8, 128))
    for p in range(NY):
        store_triple(s1_src, p, (end_state[p * 32 : p * 32 + 32], end_top, end_total))
    s1, s2, s3 = slots.take(NY), slots.take(NZ), slots.take(NY)
    for d in range(1, NY):
        send(s1_src.at[y_at[d]], s1_buf.at[y], s1 + d, {"y": y_at[d]})
    s1_buf[y] = s1_src[y]
    gu_y_send(0)
    gu_z_wait(0)
    gu_z_send(1)
    gu_y_send(1)
    dn_y_forward()

    top_cols = as_columns(top_run)
    step_rows = 256

    def local_rows(i):
        r0 = i * step_rows
        top_tile = top_cols[r0 : r0 + step_rows]
        parts = None
        for j in range(i + 1):
            s0 = j * step_rows
            scores = lax.dot_general(
                q_ref[r0 : r0 + step_rows], k_ref[s0 : s0 + step_rows],
                (((1,), (1,)), ((), ())), preferred_element_type=F32,
            )
            log_weight = lead[:, s0 : s0 + step_rows] - wide(top_tile, step_rows // 128)
            if i == j:
                at_row = lax.broadcasted_iota(jnp.int32, (step_rows, step_rows), 0)
                at_col = lax.broadcasted_iota(jnp.int32, (step_rows, step_rows), 1)
                log_weight = jnp.where(at_col <= at_row, log_weight, -jnp.inf)
            scores = (scores * (128.0**-0.5) * jnp.exp(log_weight)).astype(BF16)
            term = jnp.dot(scores, v_ref[s0 : s0 + step_rows], preferred_element_type=F32)
            parts = term if parts is None else parts + term
        num_ref[r0 : r0 + step_rows, :] = parts

    local_rows(0)
    local_rows(1)

    for d in range(1, NY):
        arrived(s1_buf.at[y_at[NY - d]], s1 + d)
    inside = [load_triple(s1_buf, 0)]
    for j in range(1, NY):
        inside.append(join(inside[-1], load_triple(s1_buf, j)))
    store_triple(s2_src, 0, inside[-1])
    for d in range(1, NZ):

        @pl.when(z + d < NZ)
        def _(d=d):
            pltpu.make_async_remote_copy(
                src_ref=s2_src.at[0], dst_ref=s2_buf.at[z], send_sem=ssem.at[s2 + d],
                recv_sem=rsem.at[s2 + d], device_id={"z": z_at[d]}, device_id_type=MESH,
            ).start()

    local_rows(2)
    local_rows(3)
    gu_z_wait(1)
    gu_z_send(2)
    gu_y_send(2)
    for d in range(1, NZ):

        @pl.when(z - d >= 0)
        def _(d=d):
            arrived(s2_buf.at[z_at[NZ - d]], s2 + d)

    before = load_triple(s2_buf, 0)
    for j in range(1, NZ):
        before = join(before, load_triple(s2_buf, j))
    store_triple(s3_src, 0, before)
    for j in range(1, NY):
        store_triple(s3_src, j, join(before, inside[j - 1]))
    for d in range(1, NY):
        send(s3_src.at[y_at[d]], s3_buf.at[y], s3 + d, {"y": y_at[d]})
    s3_buf[y] = s3_src[y]
    dn_y_wait()
    gu_z_wait(2)
    gu_z_send(3)
    dn_z_send(0)
    for d in range(1, NY):
        arrived(s3_buf.at[y_at[NY - d]], s3 + d)
    for p in range(NY):
        state_ref[p * 32 : p * 32 + 32, :] = s3_buf[p, 0:32, :].astype(BF16)
    carried_top = s3_buf[0, 32:33, 0:128]

    def reduce_slots():
        return [slots.take(7) for _ in range(CHUNKS)]

    sums = (reduce_slots(), reduce_slots())
    gathers = [slots.take(8) for _ in range(CHUNKS)]

    def swap_send(a, i):
        send(pbuf.at[a, i, other], prcv.at[a, i], sums[a][i], to_mate)

    def swap_join(a, i):
        n = sums[a][i]
        arrived(prcv.at[a, i], n)
        for j in range(NX):
            both = pbuf[a, i, c, j].astype(F32) + prcv[a, i, j].astype(F32)
            qbuf[a, i, j] = both.astype(BF16)
        top, low = pl.ds(0, half), pl.ds(half, half)
        send(qbuf.at[a, i, x_at[2], top], rly.at[a, i, 0], n + 1, to_right)
        send(qbuf.at[a, i, x_at[2], low], rly.at[a, i, 1], n + 2, to_left)
        send(qbuf.at[a, i, x_at[1], low], fin.at[a, i, 0, 1], n + 3, to_right)
        send(qbuf.at[a, i, x_at[3], top], fin.at[a, i, 1, 0], n + 4, to_left)

    def relay(a, i):
        n = sums[a][i]
        arrived(rly.at[a, i, 0], n + 1)
        added = rly[a, i, 0].astype(F32) + qbuf[a, i, x_at[1], 0:half].astype(F32)
        rsum[a, i, 0] = added.astype(BF16)
        send(rsum.at[a, i, 0], fin.at[a, i, 0, 0], n + 5, to_right)
        arrived(rly.at[a, i, 1], n + 2)
        added = rly[a, i, 1].astype(F32) + qbuf[a, i, x_at[3], half:].astype(F32)
        rsum[a, i, 1] = added.astype(BF16)
        send(rsum.at[a, i, 1], fin.at[a, i, 1, 1], n + 6, to_left)

    def total(a, i):
        n = sums[a][i]
        arrived(fin.at[a, i, 0, 1], n + 3)
        arrived(fin.at[a, i, 1, 0], n + 4)
        arrived(fin.at[a, i, 0, 0], n + 5)
        arrived(fin.at[a, i, 1, 1], n + 6)
        found = []
        for h in range(2):
            own = qbuf[a, i, x, h * half : h * half + half].astype(F32)
            found.append(own + fin[a, i, 0, h].astype(F32) + fin[a, i, 1, h].astype(F32))
        return jnp.concatenate(found, axis=0)

    def gated_chunk(i):
        r0 = i * chunk
        part = pl.ds(r0, chunk)
        run = top_cols[r0 : r0 + chunk]
        top = jnp.maximum(run, carried_top)
        keep = wide(jnp.exp(run - top), 2)
        enter = wide(jnp.exp(carried_top - top) * (128.0**-0.5), 2)
        earlier = jnp.dot(q_ref[part], state_ref[...], preferred_element_type=F32)
        memory = keep * num_ref[part] + enter * earlier
        mean = jnp.mean(memory * memory, axis=1, keepdims=True)
        opened = jax.nn.sigmoid(og_ref[part].astype(F32))
        gated = memory * lax.rsqrt(mean + EPSILON) * hg_ref[...].astype(F32) * opened
        gated = gated.astype(BF16)
        for b in range(2 * NX):
            term = jnp.dot(
                gated, wo_ref[:, b * 256 : b * 256 + 256], preferred_element_type=F32
            )
            pbuf[0, i, b % 2, b // 2] = term.astype(BF16)
        swap_send(0, i)

    def stream_chunk(i):
        n = gathers[i]
        summed = total(0, i) + res_ref[pl.ds(i * chunk, chunk)].astype(F32)
        sbuf[i, x, c] = summed.astype(BF16)
        at = sbuf.at[i, x, c]
        send(at, at, n, to_right)
        send(at, at, n + 1, to_left)
        send(at, at, n + 2, to_mate)

    def spread_chunk(i):
        n = gathers[i]
        arrived(sbuf.at[i, x_at[3], c], n)
        at = sbuf.at[i, x_at[3], c, pl.ds(0, half)]
        send(at, at, n + 3, to_right)
        at = sbuf.at[i, x_at[3], c]
        send(at, at, n + 5, to_mate)
        arrived(sbuf.at[i, x_at[1], c], n + 1)
        at = sbuf.at[i, x_at[1], c, pl.ds(half, half)]
        send(at, at, n + 4, to_left)
        at = sbuf.at[i, x_at[1], c]
        send(at, at, n + 6, to_mate)

    def far_chunk(i):
        n = gathers[i]
        arrived(sbuf.at[i, x_at[2], c, pl.ds(0, half)], n + 3)
        arrived(sbuf.at[i, x_at[2], c, pl.ds(half, half)], n + 4)
        at = sbuf.at[i, x_at[2], c]
        send(at, at, n + 7, to_mate)

    def normed_chunk(i):
        n = gathers[i]
        for d, number in ((0, n + 2), (3, n + 5), (1, n + 6), (2, n + 7)):
            arrived(sbuf.at[i, x_at[d], other], number)
        square = jnp.zeros((chunk, 256), F32)
        for b in range(2 * NX):
            part = sbuf[i, b // 2, b % 2].astype(F32)
            square = square + part * part
        mean = jnp.sum(square, axis=1, keepdims=True) * (1.0 / (2 * NX * 256))
        scale = lax.rsqrt(mean + EPSILON)
        for b in range(2 * NX):
            cols = slice(b * 256, b * 256 + 256)
            part = sbuf[i, b // 2, b % 2].astype(F32)
            nbuf[i, :, cols] = (part * scale * ng_ref[:, cols].astype(F32)).astype(BF16)

    def pump(tick):
        if tick == 0:
            gu_y_send(3)
            gu_y_send(4)
        elif tick == 1:
            gu_z_wait(3)
            gu_y_send(5)
            gu_y_send(6)
            gu_y_send(7)
        elif tick == 2:
            dn_z_wait(0)
            dn_z_send(1)
            for k in range(2):
                gu_y_forward(k)
        elif tick == 4:
            dn_z_wait(1)
            dn_z_send(2)
            for k in range(2, 4):
                gu_y_forward(k)
        elif tick == 5:
            for k in range(4, 6):
                gu_y_forward(k)
        elif tick == 6:
            dn_z_wait(2)
            dn_z_send(3)
        elif tick == 7:
            gu_y_forward(6)
            gu_y_forward(7)

    for i in range(CHUNKS):
        gated_chunk(i)
    stages = (
        lambda i: swap_join(0, i), lambda i: relay(0, i), stream_chunk,
        spread_chunk, far_chunk, normed_chunk,
    )
    for tick in range(CHUNKS + len(stages) - 1):
        for lag in range(len(stages)):
            if 0 <= tick - lag < CHUNKS:
                stages[lag](tick - lag)
        pump(tick)

    for k in range(8):
        gu_y_wait(k)

    def up_cols(i, col, width):
        weights = gu_all[:, :, col : col + width].reshape(NZ * NY * 64, width)
        return jnp.dot(nbuf[i], weights, preferred_element_type=F32)

    def silu(v):
        return v / (1.0 + jnp.exp(-v))

    for i in range(CHUNKS):
        for col in (0, 256):
            hidden = silu(up_cols(i, col, 256)) * up_cols(i, 768 + col, 256)
            hbuf[i, :, col : col + 256] = hidden.astype(BF16)
        tail = up_cols(i, 512, 256)
        hidden = silu(tail[:, :128]) * up_cols(i, 1280, 128)
        hbuf[i, :, 512:640] = hidden.astype(BF16)
        mixed_tile = tail[:, 128:]
        hidden = silu(mixed_tile) * pltpu.roll(mixed_tile, 64, 1)
        lane = lax.broadcasted_iota(jnp.int32, hidden.shape, 1)
        hbuf[i, :, 640:768] = jnp.where(lane < 64, hidden, 0.0).astype(BF16)

    dn_z_wait(3)

    def down_chunk(i):
        for b in range(2 * NX):
            weights = dn_all[b * 4 : b * 4 + 4].reshape(256, dn_all.shape[2])
            term = lax.dot_general(
                hbuf[i], weights, (((1,), (1,)), ((), ())), preferred_element_type=F32
            )
            pbuf[1, i, b % 2, b // 2] = term.astype(BF16)
        swap_send(1, i)

    def mixed_chunk(i):
        summed = sbuf[i, x, c].astype(F32) + 0.5 * total(1, i)
        out_ref[pl.ds(i * chunk, chunk)] = summed.astype(BF16)

    stages = (down_chunk, lambda i: swap_join(1, i), lambda i: relay(1, i), mixed_chunk)
    for tick in range(CHUNKS + len(stages) - 1):
        for lag in range(len(stages)):
            if 0 <= tick - lag < CHUNKS:
                stages[lag](tick - lag)

    for copy in sends:
        copy.wait_send()
    for d in range(1, NZ):

        @pl.when(z + d < NZ)
        def _(d=d):
            pltpu.make_async_remote_copy(
                src_ref=s2_src.at[0], dst_ref=s2_buf.at[z], send_sem=ssem.at[s2 + d],
                recv_sem=rsem.at[s2 + d], device_id={"z": z_at[d]}, device_id_type=MESH,
            ).wait_send()


SEMAPHORES = 192


def local(
    queries,
    cell_key_rows,
    cell_value_rows,
    output_gate_logits,
    input_gate_logits,
    forget_gate_logits,
    forget_extra_term,
    residual,
    head_norm_gain,
    cell_output_weight,
    feedforward_norm_gain,
    gate_projection_weight,
    up_projection_weight,
    down_projection_weight,
):
    gate, up, down = gate_projection_weight, up_projection_weight, down_projection_weight
    gate_up = jnp.concatenate([gate, up[:, 640:], up[:, :640]], axis=1)
    down_rows = jnp.pad(down.T, ((0, 0), (0, 64)))
    rows = queries.shape[0]
    chunk = rows // CHUNKS
    half = chunk // 2
    vmem = pltpu.VMEM
    scratch = [
        vmem((NZ * NY, 64, 1408), BF16),
        vmem((NZ * NY, 64, 768), BF16),
        vmem((NY, 40, 256), F32),
        vmem((NY, 40, 256), F32),
        vmem((1, 40, 256), F32),
        vmem((NZ, 40, 256), F32),
        vmem((NY, 40, 256), F32),
        vmem((NY, 40, 256), F32),
        vmem((128, 256), BF16),
        vmem((rows, 256), F32),
        vmem((2, CHUNKS, 2, NX, chunk, 256), BF16),
        vmem((2, CHUNKS, NX, chunk, 256), BF16),
        vmem((2, CHUNKS, NX, chunk, 256), BF16),
        vmem((2, CHUNKS, 2, half, 256), BF16),
        vmem((2, CHUNKS, 2, half, 256), BF16),
        vmem((2, CHUNKS, 2, 2, half, 256), BF16),
        vmem((CHUNKS, NX, 2, chunk, 256), BF16),
        vmem((CHUNKS, chunk, 2048), BF16),
        vmem((CHUNKS, chunk, 768), BF16),
        pltpu.SemaphoreType.DMA((SEMAPHORES,)),
        pltpu.SemaphoreType.DMA((SEMAPHORES,)),
    ]
    return pl.pallas_call(
        cell_kernel,
        out_shape=jax.ShapeDtypeStruct(residual.shape, BF16),
        in_specs=[pl.BlockSpec(memory_space=pltpu.VMEM)] * 13,
        out_specs=pl.BlockSpec(memory_space=pltpu.VMEM),
        scratch_shapes=scratch,
        compiler_params=pltpu.CompilerParams(
            collective_id=0, has_side_effects=True, vmem_limit_bytes=62 * 1024 * 1024
        ),
    )(
        queries,
        cell_key_rows,
        cell_value_rows,
        output_gate_logits,
        input_gate_logits,
        forget_gate_logits,
        forget_extra_term,
        residual,
        head_norm_gain.reshape(1, -1),
        cell_output_weight,
        feedforward_norm_gain.reshape(1, -1),
        gate_up,
        down_rows,
    )


def solution(mesh):
    torus = Mesh(mesh.devices.reshape(NZ, NY, NX, 2), ("z", "y", "x", "c"))
    seq, head = ("z", "y"), ("x", "c")
    in_specs = (
        P(seq, head),
        P(seq, head),
        P(seq, head),
        P(seq, head),
        P(head, seq),
        P(head, seq),
        P(head, seq),
        P(seq, head),
        P(head),
        P(head, None),
        P(),
        P(seq, head),
        P(seq, head),
        P(head, seq),
    )
    return jax.shard_map(
        local, mesh=torus, in_specs=in_specs, out_specs=P(seq, head), check_vma=False
    )
```

```python
import jax
import jax.numpy as jnp
from jax import lax
from jax.experimental import pallas as pl
from jax.experimental.pallas import tpu as pltpu
from jax.sharding import Mesh
from jax.sharding import PartitionSpec as P

MESH = pl.DeviceIdType.MESH
F32 = jnp.float32
BF16 = jnp.bfloat16
LOWEST_LOG = -1e30
EPSILON = 1e-06
NZ, NY, NX = 8, 4, 4
CHUNKS = 8
BLOCKS = 4
PER_BLOCK = CHUNKS // BLOCKS
BLOCK = 256


class Slots:
    def __init__(self):
        self.used = 0

    def take(self, count=1):
        first = self.used
        self.used += count
        return first


def running_rows(row, combine, identity):
    length = row.shape[1]
    lane = lax.broadcasted_iota(jnp.int32, row.shape, 1)
    step = 1
    while step < length:
        moved = jnp.where(lane >= step, pltpu.roll(row, step, 1), identity)
        row = combine(row, moved)
        step *= 2
    return row


def as_columns(row):
    return jnp.broadcast_to(row, (128, row.shape[1])).T


def wide(tile, copies):
    return jnp.concatenate([tile] * copies, axis=1)


def join(early, late):
    state_early, top_early, total_early = early
    state_late, top_late, total_late = late
    moved = top_early + total_late
    top = jnp.maximum(moved, top_late)
    left = wide(jnp.exp(moved - top), 2)
    right = wide(jnp.exp(top_late - top), 2)
    return (left * state_early + right * state_late, top, total_early + total_late)


def in_three(value):
    high = value.astype(BF16).astype(F32)
    middle = (value - high).astype(BF16).astype(F32)
    low = value - high - middle
    at = lax.broadcasted_iota(jnp.int32, (16, 128), 0)
    tile = jnp.where(at == 0, high, jnp.where(at == 1, middle, jnp.where(at == 2, low, 0.0)))
    return tile.astype(BF16)


def load_triple(ref, index):
    part = ref[index].astype(F32)
    scalars = part[32:33] + part[33:34] + part[34:35]
    return (part[0:32], scalars[:, 0:128], scalars[:, 128:256])


def store_triple(ref, index, triple):
    state, top, total = triple
    ref[index, 0:32, :] = state.astype(BF16)
    ref[index, 32:48, 0:128] = in_three(top)
    ref[index, 32:48, 128:256] = in_three(total)


def cell_kernel(
    q_in, k_in, v_in, og_in, ig_in, fg_in, ex_in, res_in, hg_in, wo_in, ng_in,
    gate_in, up_in, down_in,
    out_hbm,
    q_ref, k_ref, v_ref, og_ref, ig_ref, fg_ref, ex_ref, res_ref, hg_ref, wo_ref, ng_ref,
    gate_ref, up_ref, down_ref, out_ref,
    gu_all, dn_all, s1_src, s1_buf, s2_src, s2_buf, s3_src, s3_buf, state_ref,
    num_ref, pbuf, prcv, qbuf, rly, rsum, fin, sbuf, nbuf, hbuf,
    ssem, rsem, isem, osem,
):
    z, y, x, c = (lax.axis_index(a) for a in ("z", "y", "x", "c"))
    rows = q_ref.shape[0]
    chunk = rows // CHUNKS
    half = chunk // 2
    other = 1 - c
    x_at = [lax.rem(x + d, NX) for d in range(NX)]
    y_at = [lax.rem(y + d, NY) for d in range(NY)]
    z_at = [lax.rem(z + d, NZ) for d in range(NZ)]
    to_right, to_left, to_mate = {"x": x_at[1]}, {"x": x_at[3]}, {"c": other}
    y_right, y_left = {"y": y_at[1]}, {"y": y_at[3]}
    z_right, z_left = {"z": z_at[1]}, {"z": z_at[7]}
    stores, slots = [], Slots()

    def remote(src, dst, group, number, device):
        return pltpu.make_async_remote_copy(
            src_ref=src, dst_ref=dst, send_sem=ssem.at[group], recv_sem=rsem.at[number],
            device_id=device, device_id_type=MESH,
        )

    def send(src, dst, number, device, group):
        remote(src, dst, group, number, device).start()

    def arrived(dst, number):
        remote(dst, dst, 0, number, to_mate).wait_recv()

    def left(src, group):
        remote(src, src, group, 0, to_mate).wait_send()

    sums_out, gather_out, gu_out, dn_out, s1_out, s3_out, s2_out = (0, 1), 2, 3, 4, 5, 6, 7

    own = z * NY + y

    loads = {}
    for number, (name, src, dst) in enumerate((
        ("gate", gate_in, gate_ref), ("up", up_in, up_ref), ("down", down_in, down_ref),
        ("ig", ig_in, ig_ref), ("fg", fg_in, fg_ref), ("ex", ex_in, ex_ref),
        ("k", k_in, k_ref), ("v", v_in, v_ref), ("q", q_in, q_ref),
        ("hg", hg_in, hg_ref), ("ng", ng_in, ng_ref), ("og", og_in, og_ref),
        ("wo", wo_in, wo_ref), ("res", res_in, res_ref),
    )):
        loads[name] = pltpu.make_async_copy(src, dst, isem.at[number])

    def loaded(*names):
        for name in names:
            loads[name].wait()

    def enter():
        low = jnp.full((1, 128), LOWEST_LOG, F32)
        for j in range(NZ):
            store_triple(s2_buf, j, (jnp.zeros((32, 256), F32), low, jnp.zeros((1, 128), F32)))
        for copy in loads.values():
            copy.start()
        for device in partners:
            pl.semaphore_signal(barrier, inc=1, device_id=device, device_id_type=MESH)

    def lay_weights():
        loaded("gate", "up", "down")
        gate, up, down = gate_ref[...], up_ref[...], down_ref[...]
        gu_all[own, :, 0:640] = gate[:, 0:640]
        gu_all[own, :, 640:768] = jnp.concatenate([gate[:, 640:704], up[:, 640:704]], axis=1)
        gu_all[own, :, 768:1408] = up[:, 0:640]
        dn_all[own, :, 0:640] = down[:, 0:640]
        dn_all[own, :, 640:768] = jnp.concatenate(
            [down[:, 640:704], jnp.zeros((64, 64), BF16)], axis=1
        )

    barrier = pltpu.get_barrier_semaphore()
    partners = [to_right, to_left, to_mate]
    partners += [{"y": y_at[d]} for d in range(1, NY)] + [{"z": z_at[d]} for d in range(1, NZ)]

    def meet():
        pl.semaphore_wait(barrier, len(partners))

    gz_r, gz_l = slots.take(4), slots.take(4)
    gy_r, gy_l, gy_far = slots.take(8), slots.take(8), slots.take(1)
    dy = slots.take(3)
    dz_r, dz_l = slots.take(4), slots.take(3)
    z_order = [0, 7, 1, 6, 2, 5, 3, 4]
    piece = gu_all.shape[1] // 2

    def gu_z_send(step):
        if step == 0:
            at = gu_all.at[own]
            send(at, at, gz_r, z_right, gu_out)
            send(at, at, gz_l, z_left, gu_out)
        elif step < 3:
            for number, d, device in ((gz_r, NZ - step, z_right), (gz_l, step, z_left)):
                at = gu_all.at[z_at[d] * NY + y]
                send(at, at, number + step, device, gu_out)
        else:
            at = gu_all.at[z_at[5] * NY + y, pl.ds(0, piece)]
            send(at, at, gz_r + 3, z_right, gu_out)
            at = gu_all.at[z_at[3] * NY + y, pl.ds(piece, piece)]
            send(at, at, gz_l + 3, z_left, gu_out)

    def gu_z_wait(step):
        if step < 3:
            arrived(gu_all.at[z_at[7 - step] * NY + y], gz_r + step)
            arrived(gu_all.at[z_at[1 + step] * NY + y], gz_l + step)
        else:
            arrived(gu_all.at[z_at[4] * NY + y, pl.ds(0, piece)], gz_r + 3)
            arrived(gu_all.at[z_at[4] * NY + y, pl.ds(piece, piece)], gz_l + 3)

    def gu_y_send(k):
        at = gu_all.at[z_at[z_order[k]] * NY + y]
        send(at, at, gy_r + k, y_right, gu_out)
        send(at, at, gy_l + k, y_left, gu_out)

    def gu_y_forward(k):
        block = z_at[z_order[k]] * NY
        arrived(gu_all.at[block + y_at[3]], gy_r + k)
        at = gu_all.at[block + y_at[3], pl.ds(0, piece)]
        send(at, at, gy_far, y_right, gu_out)
        arrived(gu_all.at[block + y_at[1]], gy_l + k)
        at = gu_all.at[block + y_at[1], pl.ds(piece, piece)]
        send(at, at, gy_far, y_left, gu_out)

    def gu_y_wait():
        arrived(gu_all.at[pl.ds(0, NZ)], gy_far)

    def dn_y_send():
        at = dn_all.at[own]
        send(at, at, dy, y_right, dn_out)
        send(at, at, dy + 1, y_left, dn_out)

    def dn_y_forward():
        arrived(dn_all.at[z * NY + y_at[3]], dy)
        at = dn_all.at[z * NY + y_at[3], pl.ds(0, piece)]
        send(at, at, dy + 2, y_right, dn_out)
        arrived(dn_all.at[z * NY + y_at[1]], dy + 1)
        at = dn_all.at[z * NY + y_at[1], pl.ds(piece, piece)]
        send(at, at, dy + 2, y_left, dn_out)

    def dn_y_wait():
        arrived(dn_all.at[z * NY + y_at[2]], dy + 2)

    def dn_z_send(step):
        if step < 3:
            for number, d, device in ((dz_r, (NZ - step) % NZ, z_right), (dz_l, step, z_left)):
                at = dn_all.at[pl.ds(z_at[d] * NY, NY)]
                send(at, at, number + step, device, dn_out)
        else:
            at = dn_all.at[pl.ds(z_at[5] * NY, 2)]
            send(at, at, dz_r + 3, z_right, dn_out)
            at = dn_all.at[pl.ds(z_at[3] * NY + 2, 2)]
            send(at, at, dz_r + 3, z_left, dn_out)

    def dn_z_wait(step):
        if step < 3:
            arrived(dn_all.at[pl.ds(z_at[7 - step] * NY, NY)], dz_r + step)
            arrived(dn_all.at[pl.ds(z_at[1 + step] * NY, NY)], dz_l + step)
        else:
            arrived(dn_all.at[pl.ds(z_at[4] * NY, NY)], dz_r + 3)

    def gates():
        loaded("ig", "fg", "ex")
        logits = fg_ref[...].astype(F32)
        log_forget = jnp.minimum(logits, 0.0) - jnp.log1p(jnp.exp(-jnp.abs(logits))) + ex_ref[...]
        cum = running_rows(log_forget, jnp.add, 0.0)
        lead = ig_ref[...].astype(F32) - cum
        return cum, lead, running_rows(lead, jnp.maximum, -jnp.inf)

    s1, s2, s3 = slots.take(), slots.take(NZ - 1) - 1, slots.take()

    def end_parts():
        loaded("k", "v")
        last_cum, last_lead = cum[:, rows - 1 :], top_run[:, rows - 1 :]
        weight = as_columns(jnp.exp(lead - last_lead))
        scaled = (k_ref[...].astype(F32) * weight).astype(BF16)
        end_state = lax.dot_general(
            scaled, v_ref[...], (((0,), (0,)), ((), ())), preferred_element_type=F32
        )
        end_top = jnp.broadcast_to(last_cum + last_lead, (1, 128))
        end_total = jnp.broadcast_to(last_cum, (1, 128))
        for p in range(NY):
            store_triple(s1_src, p, (end_state[p * 32 : p * 32 + 32], end_top, end_total))
        s1_buf[y] = s1_src[y]

    def send_parts():
        for d in range(1, NY):
            send(s1_src.at[y_at[d]], s1_buf.at[y], s1, {"y": y_at[d]}, s1_out)

    step_rows = 256

    def local_rows(i):
        r0 = i * step_rows
        top_tile = top_cols[r0 : r0 + step_rows]
        parts = None
        for j in range(i + 1):
            s0 = j * step_rows
            scores = lax.dot_general(
                q_ref[r0 : r0 + step_rows], k_ref[s0 : s0 + step_rows],
                (((1,), (1,)), ((), ())), preferred_element_type=F32,
            )
            log_weight = lead[:, s0 : s0 + step_rows] - wide(top_tile, step_rows // 128)
            if i == j:
                at_row = lax.broadcasted_iota(jnp.int32, (step_rows, step_rows), 0)
                at_col = lax.broadcasted_iota(jnp.int32, (step_rows, step_rows), 1)
                log_weight = jnp.where(at_col <= at_row, log_weight, -jnp.inf)
            scores = (scores * (128.0**-0.5) * jnp.exp(log_weight)).astype(BF16)
            term = jnp.dot(scores, v_ref[s0 : s0 + step_rows], preferred_element_type=F32)
            parts = term if parts is None else parts + term
        num_ref[r0 : r0 + step_rows, :] = parts

    def state_copy(d):
        return remote(s2_src.at[0], s2_buf.at[z], s2_out + d - 1, s2 + d, {"z": z_at[d]})

    def y_states():
        arrived(s1_buf.at[pl.ds(0, NY - 1)], s1)
        inside = [load_triple(s1_buf, 0)]
        for j in range(1, NY):
            inside.append(join(inside[-1], load_triple(s1_buf, j)))
        store_triple(s2_src, 0, inside[-1])
        for d in range(1, NZ):

            @pl.when(z + d < NZ)
            def _(d=d):
                state_copy(d).start()

        return inside

    def z_states():
        for d in range(1, NZ):

            @pl.when(z - d >= 0)
            def _(d=d):
                arrived(s2_buf.at[z_at[NZ - d]], s2 + d)

        before = load_triple(s2_buf, 0)
        for j in range(1, NZ):
            before = join(before, load_triple(s2_buf, j))
        store_triple(s3_src, 0, before)
        for j in range(1, NY):
            store_triple(s3_src, j, join(before, inside[j - 1]))
        for d in range(1, NY):
            send(s3_src.at[y_at[d]], s3_buf.at[y], s3, {"y": y_at[d]}, s3_out)
        s3_buf[y] = s3_src[y]

    def carried():
        arrived(s3_buf.at[pl.ds(0, NY - 1)], s3)
        for p in range(NY):
            state_ref[p * 32 : p * 32 + 32, :] = s3_buf[p, 0:32, :]
        return load_triple(s3_buf, 0)[1]

    enter()
    lay_weights()
    cum, lead, top_run = gates()
    end_parts()
    meet()
    send_parts()
    gu_z_send(0)
    top_cols = as_columns(top_run)
    loaded("q", "hg", "ng", "og", "wo", "res")
    head_gain = hg_ref[...].astype(F32).reshape(1, 256)
    feed_gain = ng_ref[...].astype(F32).reshape(1, 2048)
    for i in range(4):
        local_rows(i)
    inside = y_states()
    dn_y_send()
    gu_y_send(0)
    gu_z_wait(0)
    gu_z_send(1)
    z_states()
    gu_y_send(1)
    gu_y_send(2)
    dn_y_forward()
    carried_top = carried()

    def reduce_slots():
        return [slots.take(4) for _ in range(CHUNKS)]

    sums = (reduce_slots(), reduce_slots())
    gathers = [slots.take(4) for _ in range(CHUNKS)]

    def swap_send(a, i):
        send(pbuf.at[a, i, other], prcv.at[a, i], sums[a][i], to_mate, sums_out[a])

    def swap_join(a, i):
        n = sums[a][i]
        arrived(prcv.at[a, i], n)
        for j in range(NX):
            both = pbuf[a, i, c, j].astype(F32) + prcv[a, i, j].astype(F32)
            qbuf[a, i, j] = both.astype(BF16)
        top, low = pl.ds(0, half), pl.ds(half, half)
        send(qbuf.at[a, i, x_at[2], top], rly.at[a, i, 0], n + 1, to_right, sums_out[a])
        send(qbuf.at[a, i, x_at[2], low], rly.at[a, i, 1], n + 2, to_left, sums_out[a])
        send(qbuf.at[a, i, x_at[1], low], fin.at[a, i, 0, 1], n + 3, to_right, sums_out[a])
        send(qbuf.at[a, i, x_at[3], top], fin.at[a, i, 1, 0], n + 3, to_left, sums_out[a])

    def relay(a, i):
        n = sums[a][i]
        arrived(rly.at[a, i, 0], n + 1)
        added = rly[a, i, 0].astype(F32) + qbuf[a, i, x_at[1], 0:half].astype(F32)
        rsum[a, i, 0] = added.astype(BF16)
        send(rsum.at[a, i, 0], fin.at[a, i, 0, 0], n + 3, to_right, sums_out[a])
        arrived(rly.at[a, i, 1], n + 2)
        added = rly[a, i, 1].astype(F32) + qbuf[a, i, x_at[3], half:].astype(F32)
        rsum[a, i, 1] = added.astype(BF16)
        send(rsum.at[a, i, 1], fin.at[a, i, 1, 1], n + 3, to_left, sums_out[a])

    def total(a, i):
        n = sums[a][i]
        arrived(fin.at[a, i], n + 3)
        found = []
        for h in range(2):
            own = qbuf[a, i, x, h * half : h * half + half].astype(F32)
            found.append(own + fin[a, i, 0, h].astype(F32) + fin[a, i, 1, h].astype(F32))
        return jnp.concatenate(found, axis=0)

    def gated_block(g):
        part = pl.ds(g * BLOCK, BLOCK)
        run = top_cols[g * BLOCK : g * BLOCK + BLOCK]
        top = jnp.maximum(run, carried_top)
        keep = wide(jnp.exp(run - top), 2)
        enter = wide(jnp.exp(carried_top - top) * (128.0**-0.5), 2)
        earlier = jnp.dot(q_ref[part], state_ref[...], preferred_element_type=F32)
        memory = keep * num_ref[part] + enter * earlier
        mean = jnp.mean(memory * memory, axis=1, keepdims=True)
        opened = jax.nn.sigmoid(og_ref[part].astype(F32))
        gated = memory * lax.rsqrt(mean + EPSILON) * head_gain * opened
        gated = gated.astype(BF16)
        place(0, g, lambda b: jnp.dot(
            gated, wo_ref[:, b * 256 : b * 256 + 256], preferred_element_type=F32
        ))

    def place(a, g, term):
        for b in range(2 * NX):
            found = term(b).astype(BF16)
            for i in range(PER_BLOCK):
                pbuf[a, g * PER_BLOCK + i, b % 2, b // 2] = found[i * chunk : i * chunk + chunk]
        for i in range(PER_BLOCK):
            swap_send(a, g * PER_BLOCK + i)

    def stream_chunk(i):
        n = gathers[i]
        summed = total(0, i) + res_ref[pl.ds(i * chunk, chunk)].astype(F32)
        sbuf[i, c, x] = summed.astype(BF16)
        at = sbuf.at[i, c, x]
        send(at, at, n, to_right, gather_out)
        send(at, at, n + 1, to_left, gather_out)
        send(at, at, n + 3, to_mate, gather_out)

    def spread_chunk(i):
        n = gathers[i]
        for number, d, first, device in ((n, 3, 0, to_right), (n + 1, 1, half, to_left)):
            at = sbuf.at[i, c, x_at[d]]
            arrived(at, number)
            part = sbuf.at[i, c, x_at[d], pl.ds(first, half)]
            send(part, part, n + 2, device, gather_out)
            send(at, at, n + 3, to_mate, gather_out)

    def far_chunk(i):
        n = gathers[i]
        at = sbuf.at[i, c, x_at[2]]
        arrived(at, n + 2)
        send(at, at, n + 3, to_mate, gather_out)

    def normed_chunk(i):
        arrived(sbuf.at[i, other], gathers[i] + 3)
        square = jnp.zeros((chunk, 256), F32)
        for b in range(2 * NX):
            part = sbuf[i, b % 2, b // 2].astype(F32)
            square = square + part * part
        mean = jnp.sum(square, axis=1, keepdims=True) * (1.0 / (2 * NX * 256))
        scale = lax.rsqrt(mean + EPSILON)
        for b in range(2 * NX):
            cols = slice(b * 256, b * 256 + 256)
            part = sbuf[i, b % 2, b // 2].astype(F32)
            nbuf[pl.ds(i * chunk, chunk), cols] = (part * scale * feed_gain[:, cols]).astype(BF16)

    def pump(tick):
        if tick == 0:
            gu_z_wait(1)
            gu_z_send(2)
            gu_y_send(3)
        elif tick == 1:
            dn_y_wait()
            dn_z_send(0)
            gu_y_send(4)
        elif tick == 2:
            gu_z_wait(2)
            gu_z_send(3)
            gu_y_send(5)
            gu_y_send(6)
        elif tick == 3:
            gu_y_forward(0)
            gu_y_forward(1)
        elif tick == 4:
            dn_z_wait(0)
            dn_z_send(1)
            gu_z_wait(3)
            gu_y_send(7)
        elif tick == 5:
            gu_y_forward(2)
            gu_y_forward(3)
        elif tick == 6:
            dn_z_wait(1)
            dn_z_send(2)
            gu_y_forward(4)
        elif tick == 7:
            gu_y_forward(5)
        elif tick == 8:
            gu_y_forward(6)
        elif tick == 9:
            dn_z_wait(2)
            dn_z_send(3)
            gu_y_forward(7)

    def run(stages, pump=None):
        for tick in range(CHUNKS + max(lag for lag, _ in stages)):
            for lag, stage in stages:
                if 0 <= tick - lag < CHUNKS:
                    stage(tick - lag)
            if pump is not None:
                pump(tick)

    def first_of_block(stage):
        def begin(i):
            if i % PER_BLOCK == 0:
                stage(i // PER_BLOCK)

        return begin

    def join_first(i):
        swap_join(0, i)

    def relay_first(i):
        relay(0, i)

    run(
        (
            (0, first_of_block(gated_block)), (1, join_first), (2, relay_first),
            (3, stream_chunk), (4, spread_chunk), (5, far_chunk), (6, normed_chunk),
        ),
        pump,
    )

    def silu(v):
        return v / (1.0 + jnp.exp(-v))

    def up_block(g):
        lines = nbuf[pl.ds(g * BLOCK, BLOCK)]
        part = pl.ds(g * BLOCK, BLOCK)

        def up_cols(col, width):
            weights = gu_all[:, :, col : col + width].reshape(NZ * NY * 64, width)
            return jnp.dot(lines, weights, preferred_element_type=F32)

        for col in (0, 256):
            hidden = silu(up_cols(col, 256)) * up_cols(768 + col, 256)
            hbuf[part, col : col + 256] = hidden.astype(BF16)
        tail = up_cols(512, 256)
        hidden = silu(tail[:, :128]) * up_cols(1280, 128)
        hbuf[part, 512:640] = hidden.astype(BF16)
        mixed_tile = tail[:, 128:]
        hidden = silu(mixed_tile) * pltpu.roll(mixed_tile, 64, 1)
        lane = lax.broadcasted_iota(jnp.int32, hidden.shape, 1)
        hbuf[part, 640:768] = jnp.where(lane < 64, hidden, 0.0).astype(BF16)

    def down_block(g):
        def term(b):
            weights = dn_all[b * 4 : b * 4 + 4].reshape(256, dn_all.shape[2])
            return lax.dot_general(
                hbuf[pl.ds(g * BLOCK, BLOCK)], weights, (((1,), (1,)), ((), ())),
                preferred_element_type=F32,
            )

        place(1, g, term)

    def mixed_chunk(i):
        summed = sbuf[i, c, x].astype(F32) + 0.5 * total(1, i)
        part = pl.ds(i * chunk, chunk)
        out_ref[part] = summed.astype(BF16)
        stores.append(pltpu.make_async_copy(out_ref.at[part], out_hbm.at[part], osem.at[i]))
        stores[-1].start()

    def feed_block(g):
        if g == 0:
            gu_y_wait()
        up_block(g)
        if g == 0:
            dn_z_wait(3)
        down_block(g)

    def join_last(i):
        swap_join(1, i)

    def relay_last(i):
        relay(1, i)

    run(((0, first_of_block(feed_block)), (1, join_last), (3, relay_last), (5, mixed_chunk)))

    def drain():
        for copy in stores:
            copy.wait()
        for group in (*sums_out, gather_out):
            left(sbuf.at[pl.ds(0, 7)], group)
        left(gu_all.at[pl.ds(0, 31)], gu_out)
        left(dn_all.at[pl.ds(0, 31)], dn_out)
        left(s1_buf.at[pl.ds(0, NY - 1)], s1_out)
        left(s3_buf.at[pl.ds(0, NY - 1)], s3_out)
        for d in range(1, NZ):

            @pl.when(z + d < NZ)
            def _(d=d):
                state_copy(d).wait_send()

    drain()
    assert slots.used <= RECEIVES


RECEIVES, SENDS = 144, 14


def local(
    queries,
    cell_key_rows,
    cell_value_rows,
    output_gate_logits,
    input_gate_logits,
    forget_gate_logits,
    forget_extra_term,
    residual,
    head_norm_gain,
    cell_output_weight,
    feedforward_norm_gain,
    gate_projection_weight,
    up_projection_weight,
    down_projection_weight,
):
    rows = queries.shape[0]
    chunk = rows // CHUNKS
    half = chunk // 2
    vmem = pltpu.VMEM
    arguments = (
        queries,
        cell_key_rows,
        cell_value_rows,
        output_gate_logits,
        input_gate_logits,
        forget_gate_logits,
        forget_extra_term,
        residual,
        head_norm_gain,
        cell_output_weight,
        feedforward_norm_gain,
        gate_projection_weight,
        up_projection_weight,
        down_projection_weight.T,
    )
    scratch = [vmem(a.shape, a.dtype) for a in arguments] + [
        vmem(residual.shape, BF16),
        vmem((NZ * NY, 64, 1408), BF16),
        vmem((NZ * NY, 64, 768), BF16),
        vmem((NY, 48, 256), BF16),
        vmem((NY, 48, 256), BF16),
        vmem((1, 48, 256), BF16),
        vmem((NZ, 48, 256), BF16),
        vmem((NY, 48, 256), BF16),
        vmem((NY, 48, 256), BF16),
        vmem((128, 256), BF16),
        vmem((rows, 256), F32),
        vmem((2, CHUNKS, 2, NX, chunk, 256), BF16),
        vmem((2, CHUNKS, NX, chunk, 256), BF16),
        vmem((2, CHUNKS, NX, chunk, 256), BF16),
        vmem((2, CHUNKS, 2, half, 256), BF16),
        vmem((2, CHUNKS, 2, half, 256), BF16),
        vmem((2, CHUNKS, 2, 2, half, 256), BF16),
        vmem((CHUNKS, 2, NX, chunk, 256), BF16),
        vmem((rows, 2048), BF16),
        vmem((rows, 768), BF16),
        pltpu.SemaphoreType.DMA((SENDS,)),
        pltpu.SemaphoreType.DMA((RECEIVES,)),
        pltpu.SemaphoreType.DMA((len(arguments),)),
        pltpu.SemaphoreType.DMA((CHUNKS,)),
    ]
    return pl.pallas_call(
        cell_kernel,
        out_shape=jax.ShapeDtypeStruct(residual.shape, BF16),
        in_specs=[pl.BlockSpec(memory_space=pl.ANY)] * 14,
        out_specs=pl.BlockSpec(memory_space=pl.ANY),
        scratch_shapes=scratch,
        compiler_params=pltpu.CompilerParams(
            collective_id=0, has_side_effects=True, vmem_limit_bytes=62 * 1024 * 1024
        ),
    )(*arguments)


def solution(mesh):
    torus = Mesh(mesh.devices.reshape(NZ, NY, NX, 2), ("z", "y", "x", "c"))
    seq, head = ("z", "y"), ("x", "c")
    in_specs = (
        P(seq, head),
        P(seq, head),
        P(seq, head),
        P(seq, head),
        P(head, seq),
        P(head, seq),
        P(head, seq),
        P(seq, head),
        P(head),
        P(head, None),
        P(),
        P(seq, head),
        P(seq, head),
        P(head, seq),
    )
    return jax.shard_map(
        local, mesh=torus, in_specs=in_specs, out_specs=P(seq, head), check_vma=False
    )
```

```python
import jax
import jax.numpy as jnp
from jax import lax
from jax.experimental import pallas as pl
from jax.experimental.pallas import tpu as pltpu
from jax.sharding import Mesh
from jax.sharding import PartitionSpec as P

MESH = pl.DeviceIdType.MESH
F32 = jnp.float32
BF16 = jnp.bfloat16
LOWEST_LOG = -1e30
EPSILON = 1e-06
NZ, NY, NX = 8, 4, 4
CHUNKS = 8
BLOCKS = 4
PER_BLOCK = CHUNKS // BLOCKS
BLOCK = 256
EARLY = 2


class Slots:
    def __init__(self):
        self.used = 0

    def take(self, count=1):
        first = self.used
        self.used += count
        return first


def running_rows(row, combine, identity):
    length = row.shape[1]
    lane = lax.broadcasted_iota(jnp.int32, row.shape, 1)
    step = 1
    while step < length:
        moved = jnp.where(lane >= step, pltpu.roll(row, step, 1), identity)
        row = combine(row, moved)
        step *= 2
    return row


def as_columns(row):
    return jnp.broadcast_to(row, (128, row.shape[1])).T


def wide(tile, copies):
    return jnp.concatenate([tile] * copies, axis=1)


def join(early, late):
    state_early, top_early, total_early = early
    state_late, top_late, total_late = late
    moved = top_early + total_late
    top = jnp.maximum(moved, top_late)
    left = wide(jnp.exp(moved - top), 2)
    right = wide(jnp.exp(top_late - top), 2)
    return (left * state_early + right * state_late, top, total_early + total_late)


def in_three(value):
    high = value.astype(BF16).astype(F32)
    middle = (value - high).astype(BF16).astype(F32)
    low = value - high - middle
    at = lax.broadcasted_iota(jnp.int32, (16, 128), 0)
    tile = jnp.where(at == 0, high, jnp.where(at == 1, middle, jnp.where(at == 2, low, 0.0)))
    return tile.astype(BF16)


def load_triple(ref, index):
    part = ref[index].astype(F32)
    scalars = part[32:33] + part[33:34] + part[34:35]
    return (part[0:32], scalars[:, 0:128], scalars[:, 128:256])


def store_triple(ref, index, triple):
    state, top, total = triple
    ref[index, 0:32, :] = state.astype(BF16)
    ref[index, 32:48, 0:128] = in_three(top)
    ref[index, 32:48, 128:256] = in_three(total)


def cell_kernel(
    q_in, k_in, v_in, og_in, ig_in, fg_in, ex_in, res_in, hg_in, wo_in, ng_in,
    gate_in, up_in, down_in,
    out_hbm,
    q_ref, k_ref, v_ref, og_ref, ig_ref, fg_ref, ex_ref, res_ref, hg_ref, wo_ref, ng_ref,
    gate_ref, up_ref, down_ref, out_ref,
    gu_all, dn_all, s1_src, s1_buf, s2_src, s2_buf, s3_src, s3_buf, state_ref,
    num_ref, pbuf, prcv, qbuf, rly, rsum, fin, sbuf, nbuf, hbuf,
    ssem, rsem, isem, osem,
):
    z, y, x, c = (lax.axis_index(a) for a in ("z", "y", "x", "c"))
    rows = q_ref.shape[0]
    chunk = rows // CHUNKS
    half = chunk // 2
    other = 1 - c
    x_at = [lax.rem(x + d, NX) for d in range(NX)]
    y_at = [lax.rem(y + d, NY) for d in range(NY)]
    z_at = [lax.rem(z + d, NZ) for d in range(NZ)]
    to_right, to_left, to_mate = {"x": x_at[1]}, {"x": x_at[3]}, {"c": other}
    y_right, y_left = {"y": y_at[1]}, {"y": y_at[3]}
    z_right, z_left = {"z": z_at[1]}, {"z": z_at[7]}
    stores, slots = [], Slots()

    def remote(src, dst, group, number, device):
        return pltpu.make_async_remote_copy(
            src_ref=src, dst_ref=dst, send_sem=ssem.at[group], recv_sem=rsem.at[number],
            device_id=device, device_id_type=MESH,
        )

    def send(src, dst, number, device, group):
        remote(src, dst, group, number, device).start()

    def arrived(dst, number):
        remote(dst, dst, 0, number, to_mate).wait_recv()

    def left(src, group):
        remote(src, src, group, 0, to_mate).wait_send()

    sums_out, gather_out, gu_out, dn_out, s1_out, s3_out, low_out, s2_out = (0, 1), 2, 3, 4, 5, 6, 7, 8

    own = z * NY + y

    loads = {}
    for number, (name, src, dst) in enumerate((
        ("gate", gate_in, gate_ref), ("up", up_in, up_ref), ("down", down_in, down_ref),
        ("ig", ig_in, ig_ref), ("fg", fg_in, fg_ref), ("ex", ex_in, ex_ref),
        ("k", k_in, k_ref), ("v", v_in, v_ref), ("q", q_in, q_ref),
        ("hg", hg_in, hg_ref), ("ng", ng_in, ng_ref), ("og", og_in, og_ref),
        ("wo", wo_in, wo_ref), ("res", res_in, res_ref),
    )):
        loads[name] = pltpu.make_async_copy(src, dst, isem.at[number])

    def loaded(*names):
        for name in names:
            loads[name].wait()

    def enter():
        low = jnp.full((1, 128), LOWEST_LOG, F32)
        for j in range(NZ):
            store_triple(s2_buf, j, (jnp.zeros((32, 256), F32), low, jnp.zeros((1, 128), F32)))
        for copy in loads.values():
            copy.start()
        for device in partners:
            pl.semaphore_signal(barrier, inc=1, device_id=device, device_id_type=MESH)

    def lay_weights():
        loaded("gate", "up", "down")
        gate, up, down = gate_ref[...], up_ref[...], down_ref[...]
        gu_all[own, :, 0:640] = gate[:, 0:640]
        gu_all[own, :, 640:768] = jnp.concatenate([gate[:, 640:704], up[:, 640:704]], axis=1)
        gu_all[own, :, 768:1408] = up[:, 0:640]
        dn_all[own, :, 0:640] = down[:, 0:640]
        dn_all[own, :, 640:768] = jnp.concatenate(
            [down[:, 640:704], jnp.zeros((64, 64), BF16)], axis=1
        )

    barrier = pltpu.get_barrier_semaphore()
    partners = [to_right, to_left, to_mate]
    partners += [{"y": y_at[d]} for d in range(1, NY)] + [{"z": z_at[d]} for d in range(1, NZ)]

    def meet():
        pl.semaphore_wait(barrier, len(partners))

    z_order = [0, 7, 1, 6, 2, 5, 3, 4]

    class ZFirst:
        def __init__(self, ref, count, group):
            self.ref, self.count, self.group = ref, count, group
            self.along_z, self.along_y, self.far = slots.take(4), slots.take(NZ), slots.take()

        def part(self, block, first, count):
            return self.ref.at[block, pl.ds(first, count)]

        def pass_on(self, at, number, device):
            send(at, at, number, device, self.group)

        def taken(self, blocks, number):
            arrived(self.ref.at[pl.ds(0, blocks), pl.ds(0, self.count)], number)

        def z_send(self, step):
            half_rows = self.count // 2
            for d, first, device in (((NZ - step) % NZ, 0, z_right), (step, half_rows, z_left)):
                block = z_at[d] * NY + y
                whole = (0, self.count) if step < 3 else (first, half_rows)
                self.pass_on(self.part(block, *whole), self.along_z + step, device)

        def z_wait(self, step):
            self.taken(2 if step < 3 else 1, self.along_z + step)

        def y_send(self, k):
            at = self.part(z_at[z_order[k]] * NY + y, 0, self.count)
            self.pass_on(at, self.along_y + k, y_right)
            self.pass_on(at, self.along_y + k, y_left)

        def y_forward(self, k):
            self.taken(2, self.along_y + k)
            block, half_rows = z_at[z_order[k]] * NY, self.count // 2
            self.pass_on(self.part(block + y_at[3], 0, half_rows), self.far, y_right)
            self.pass_on(self.part(block + y_at[1], half_rows, half_rows), self.far, y_left)

        def y_wait(self):
            self.taken(NZ, self.far)

    class YFirst:
        def __init__(self, ref, first, count, group):
            self.ref, self.first, self.count, self.group = ref, first, count, group
            self.along_y, self.far, self.along_z = slots.take(), slots.take(), slots.take(7)

        def pass_on(self, at, number, device):
            send(at, at, number, device, self.group)

        def taken(self, blocks, number):
            arrived(self.ref.at[pl.ds(0, blocks), pl.ds(self.first, self.count)], number)

        def y_send(self):
            at = self.ref.at[own, pl.ds(self.first, self.count)]
            self.pass_on(at, self.along_y, y_right)
            self.pass_on(at, self.along_y, y_left)

        def y_forward(self):
            self.taken(2, self.along_y)
            half_rows = self.count // 2
            at = self.ref.at[z * NY + y_at[3], pl.ds(self.first, half_rows)]
            self.pass_on(at, self.far, y_right)
            at = self.ref.at[z * NY + y_at[1], pl.ds(self.first + half_rows, half_rows)]
            self.pass_on(at, self.far, y_left)

        def y_wait(self):
            self.taken(1, self.far)

        def pair(self, d, part):
            return self.ref.at[pl.ds(z_at[d] * NY + 2 * part, 2), pl.ds(self.first, self.count)]

        def z_send(self, step, part):
            if step < 3:
                number = self.along_z + 2 * step + part
                self.pass_on(self.pair((NZ - step) % NZ, part), number, z_right)
                self.pass_on(self.pair(step, part), number, z_left)
            elif part == 0:
                self.pass_on(self.pair(5, 0), self.along_z + 6, z_right)
            else:
                self.pass_on(self.pair(3, 1), self.along_z + 6, z_left)

        def z_wait(self, step, part):
            self.taken(4, self.along_z + 2 * step + part)

    gu_rows = gu_all.shape[1] // 2
    top_gu = ZFirst(gu_all, gu_rows, gu_out)
    low_gu = YFirst(gu_all, gu_rows, gu_rows, low_out)
    dn = ZFirst(dn_all, dn_all.shape[1], dn_out)

    def gates():
        loaded("ig", "fg", "ex")
        logits = fg_ref[...].astype(F32)
        log_forget = jnp.minimum(logits, 0.0) - jnp.log1p(jnp.exp(-jnp.abs(logits))) + ex_ref[...]
        cum = running_rows(log_forget, jnp.add, 0.0)
        lead = ig_ref[...].astype(F32) - cum
        return cum, lead, running_rows(lead, jnp.maximum, -jnp.inf)

    s1, s2, s3 = slots.take(), slots.take(NZ - 1) - 1, slots.take()

    def end_parts():
        loaded("k", "v")
        last_cum, last_lead = cum[:, rows - 1 :], top_run[:, rows - 1 :]
        weight = as_columns(jnp.exp(lead - last_lead))
        scaled = (k_ref[...].astype(F32) * weight).astype(BF16)
        end_state = lax.dot_general(
            scaled, v_ref[...], (((0,), (0,)), ((), ())), preferred_element_type=F32
        )
        end_top = jnp.broadcast_to(last_cum + last_lead, (1, 128))
        end_total = jnp.broadcast_to(last_cum, (1, 128))
        for p in range(NY):
            store_triple(s1_src, p, (end_state[p * 32 : p * 32 + 32], end_top, end_total))
        s1_buf[y] = s1_src[y]

    def send_parts():
        for d in range(1, NY):
            send(s1_src.at[y_at[d]], s1_buf.at[y], s1, {"y": y_at[d]}, s1_out)

    step_rows = 256

    def local_rows(i):
        r0 = i * step_rows
        top_tile = top_cols[r0 : r0 + step_rows]
        parts = None
        for j in range(i + 1):
            s0 = j * step_rows
            scores = lax.dot_general(
                q_ref[r0 : r0 + step_rows], k_ref[s0 : s0 + step_rows],
                (((1,), (1,)), ((), ())), preferred_element_type=F32,
            )
            log_weight = lead[:, s0 : s0 + step_rows] - wide(top_tile, step_rows // 128)
            if i == j:
                at_row = lax.broadcasted_iota(jnp.int32, (step_rows, step_rows), 0)
                at_col = lax.broadcasted_iota(jnp.int32, (step_rows, step_rows), 1)
                log_weight = jnp.where(at_col <= at_row, log_weight, -jnp.inf)
            scores = (scores * (128.0**-0.5) * jnp.exp(log_weight)).astype(BF16)
            term = jnp.dot(scores, v_ref[s0 : s0 + step_rows], preferred_element_type=F32)
            parts = term if parts is None else parts + term
        num_ref[r0 : r0 + step_rows, :] = parts

    def state_copy(d):
        return remote(s2_src.at[0], s2_buf.at[z], s2_out + d - 1, s2 + d, {"z": z_at[d]})

    def y_states():
        arrived(s1_buf.at[pl.ds(0, NY - 1)], s1)
        inside = [load_triple(s1_buf, 0)]
        for j in range(1, NY):
            inside.append(join(inside[-1], load_triple(s1_buf, j)))
        store_triple(s2_src, 0, inside[-1])
        for d in range(1, NZ):

            @pl.when(z + d < NZ)
            def _(d=d):
                state_copy(d).start()

        return inside

    def z_states():
        for d in range(1, NZ):

            @pl.when(z - d >= 0)
            def _(d=d):
                arrived(s2_buf.at[z_at[NZ - d]], s2 + d)

        before = load_triple(s2_buf, 0)
        for j in range(1, NZ):
            before = join(before, load_triple(s2_buf, j))
        store_triple(s3_src, 0, before)
        for j in range(1, NY):
            store_triple(s3_src, j, join(before, inside[j - 1]))
        for d in range(1, NY):
            send(s3_src.at[y_at[d]], s3_buf.at[y], s3, {"y": y_at[d]}, s3_out)
        s3_buf[y] = s3_src[y]

    def carried():
        arrived(s3_buf.at[pl.ds(0, NY - 1)], s3)
        for p in range(NY):
            state_ref[p * 32 : p * 32 + 32, :] = s3_buf[p, 0:32, :]
        return load_triple(s3_buf, 0)[1]

    enter()
    lay_weights()
    cum, lead, top_run = gates()
    end_parts()
    meet()
    send_parts()
    top_gu.z_send(0)
    low_gu.y_send()
    top_gu.y_send(0)
    top_cols = as_columns(top_run)
    loaded("q", "hg", "ng", "og", "wo", "res")
    head_gain = hg_ref[...].astype(F32).reshape(1, 256)
    feed_gain = ng_ref[...].astype(F32).reshape(1, 2048)
    for i in range(4):
        local_rows(i)
    inside = y_states()
    top_gu.z_wait(0)
    top_gu.z_send(1)
    dn.z_send(0)
    top_gu.y_send(1)
    z_states()
    low_gu.y_forward()
    top_gu.y_send(2)
    dn.y_send(0)
    carried_top = carried()

    def reduce_slots():
        return [slots.take(4) for _ in range(CHUNKS)]

    sums = (reduce_slots(), reduce_slots())
    gathers = [slots.take(4) for _ in range(CHUNKS)]

    def swap_send(a, i):
        send(pbuf.at[a, i, other], prcv.at[a, i], sums[a][i], to_mate, sums_out[a])

    def swap_join(a, i):
        n = sums[a][i]
        arrived(prcv.at[a, i], n)
        for j in range(NX):
            both = pbuf[a, i, c, j].astype(F32) + prcv[a, i, j].astype(F32)
            qbuf[a, i, j] = both.astype(BF16)
        top, low = pl.ds(0, half), pl.ds(half, half)
        send(qbuf.at[a, i, x_at[2], top], rly.at[a, i, 0], n + 1, to_right, sums_out[a])
        send(qbuf.at[a, i, x_at[2], low], rly.at[a, i, 1], n + 2, to_left, sums_out[a])
        if i < EARLY or (a == 1 and i == CHUNKS - 1):
            direct(a, i)

    def direct(a, i):
        n = sums[a][i]
        top, low = pl.ds(0, half), pl.ds(half, half)
        send(qbuf.at[a, i, x_at[1], low], fin.at[a, i, 0, 1], n + 3, to_right, sums_out[a])
        send(qbuf.at[a, i, x_at[3], top], fin.at[a, i, 1, 0], n + 3, to_left, sums_out[a])

    def relay(a, i):
        n = sums[a][i]
        arrived(rly.at[a, i, 0], n + 1)
        added = rly[a, i, 0].astype(F32) + qbuf[a, i, x_at[1], 0:half].astype(F32)
        rsum[a, i, 0] = added.astype(BF16)
        send(rsum.at[a, i, 0], fin.at[a, i, 0, 0], n + 3, to_right, sums_out[a])
        arrived(rly.at[a, i, 1], n + 2)
        added = rly[a, i, 1].astype(F32) + qbuf[a, i, x_at[3], half:].astype(F32)
        rsum[a, i, 1] = added.astype(BF16)
        send(rsum.at[a, i, 1], fin.at[a, i, 1, 1], n + 3, to_left, sums_out[a])
        if i >= EARLY and not (a == 1 and i == CHUNKS - 1):
            direct(a, i)

    def total(a, i):
        n = sums[a][i]
        arrived(fin.at[a, i], n + 3)
        found = []
        for h in range(2):
            own = qbuf[a, i, x, h * half : h * half + half].astype(F32)
            found.append(own + fin[a, i, 0, h].astype(F32) + fin[a, i, 1, h].astype(F32))
        return jnp.concatenate(found, axis=0)

    def gated_block(g):
        part = pl.ds(g * BLOCK, BLOCK)
        run = top_cols[g * BLOCK : g * BLOCK + BLOCK]
        top = jnp.maximum(run, carried_top)
        keep = wide(jnp.exp(run - top), 2)
        enter = wide(jnp.exp(carried_top - top) * (128.0**-0.5), 2)
        earlier = jnp.dot(q_ref[part], state_ref[...], preferred_element_type=F32)
        memory = keep * num_ref[part] + enter * earlier
        mean = jnp.mean(memory * memory, axis=1, keepdims=True)
        opened = jax.nn.sigmoid(og_ref[part].astype(F32))
        gated = memory * lax.rsqrt(mean + EPSILON) * head_gain * opened
        gated = gated.astype(BF16)
        def term(j, core):
            columns = pl.ds(pl.multiple_of((2 * j + core) * 256, 256), 256)
            return jnp.dot(gated, wo_ref[:, columns], preferred_element_type=F32)

        place(0, g, term)

    def place(a, g, term):
        for core in (other, c):
            for j in range(NX):
                found = term(j, core).astype(BF16)
                for i in range(PER_BLOCK):
                    pbuf[a, g * PER_BLOCK + i, core, j] = found[i * chunk : i * chunk + chunk]
            if core is other:
                for i in range(PER_BLOCK):
                    swap_send(a, g * PER_BLOCK + i)

    def stream_chunk(i):
        n = gathers[i]
        summed = total(0, i) + res_ref[pl.ds(i * chunk, chunk)].astype(F32)
        sbuf[i, c, x] = summed.astype(BF16)
        at = sbuf.at[i, c, x]
        send(at, at, n, to_right, gather_out)
        send(at, at, n + 1, to_left, gather_out)
        send(at, at, n + 3, to_mate, gather_out)

    def spread_chunk(i):
        n = gathers[i]
        for number, d, first, device in ((n, 3, 0, to_right), (n + 1, 1, half, to_left)):
            at = sbuf.at[i, c, x_at[d]]
            arrived(at, number)
            part = sbuf.at[i, c, x_at[d], pl.ds(first, half)]
            send(part, part, n + 2, device, gather_out)
            send(at, at, n + 3, to_mate, gather_out)

    def far_chunk(i):
        n = gathers[i]
        at = sbuf.at[i, c, x_at[2]]
        arrived(at, n + 2)
        send(at, at, n + 3, to_mate, gather_out)

    def normed_chunk(i):
        arrived(sbuf.at[i, other], gathers[i] + 3)
        square = jnp.zeros((chunk, 256), F32)
        for b in range(2 * NX):
            part = sbuf[i, b % 2, b // 2].astype(F32)
            square = square + part * part
        mean = jnp.sum(square, axis=1, keepdims=True) * (1.0 / (2 * NX * 256))
        scale = lax.rsqrt(mean + EPSILON)
        for b in range(2 * NX):
            cols = slice(b * 256, b * 256 + 256)
            part = sbuf[i, b % 2, b // 2].astype(F32)
            nbuf[pl.ds(i * chunk, chunk), cols] = (part * scale * feed_gain[:, cols]).astype(BF16)

    def pump(tick):
        if tick == 0:
            top_gu.z_wait(1)
            top_gu.z_send(2)
            low_gu.y_wait()
            low_gu.z_send(0, 0)
            top_gu.y_send(3)
            top_gu.y_send(4)
            dn.z_wait(0)
            dn.z_send(1)
        elif tick == 1:
            low_gu.z_send(0, 1)
        elif tick == 2:
            top_gu.y_forward(0)
            dn.y_send(1)
        elif tick == 3:
            top_gu.z_wait(2)
            top_gu.z_send(3)
            top_gu.y_send(5)
            top_gu.y_send(6)
            top_gu.y_forward(1)
        elif tick == 4:
            dn.z_wait(1)
            dn.z_send(2)
            dn.y_send(2)
            top_gu.y_forward(2)
            top_gu.y_forward(3)
            low_gu.z_wait(0, 0)
            low_gu.z_send(1, 0)
        elif tick == 5:
            top_gu.z_wait(3)
            top_gu.y_send(7)
            low_gu.z_wait(0, 1)
            low_gu.z_send(1, 1)
            top_gu.y_forward(4)
            dn.y_send(3)
        elif tick == 6:
            dn.z_wait(2)
            dn.z_send(3)
            top_gu.y_forward(5)
            top_gu.y_forward(6)
            dn.y_send(4)
            dn.y_forward(0)
            low_gu.z_wait(1, 0)
            low_gu.z_send(2, 0)
        elif tick == 7:
            low_gu.z_wait(1, 1)
            low_gu.z_send(2, 1)
            top_gu.y_forward(7)
            dn.y_send(5)
            dn.y_send(6)
            dn.y_forward(1)
        elif tick == 8:
            low_gu.z_wait(2, 0)
            low_gu.z_send(3, 0)
            dn.z_wait(3)
            dn.y_send(7)
            dn.y_forward(2)
        elif tick == 9:
            low_gu.z_wait(2, 1)
            low_gu.z_send(3, 1)
            dn.y_forward(3)
            dn.y_forward(4)
        elif tick == 10:
            dn.y_forward(5)
        elif tick == 11:
            dn.y_forward(6)
            dn.y_forward(7)
            gu_wait()
            up_block(0)
        elif tick == 12:
            up_block(1)

    def gu_wait():
        low_gu.taken(4, low_gu.along_z + 6)
        top_gu.y_wait()

    def dn_wait():
        dn.y_wait()

    def run(stages, pump=None):
        for tick in range(CHUNKS + max(lag for lag, _ in stages)):
            for lag, stage in stages:
                if 0 <= tick - lag < CHUNKS:
                    stage(tick - lag)
            if pump is not None:
                pump(tick)

    def join_first(i):
        swap_join(0, i)

    def relay_first(i):
        relay(0, i)

    def some_gated(i):
        if i < BLOCKS:
            gated_block(i)

    def silu(v):
        return v / (1.0 + jnp.exp(-v))

    def up_block(g):
        lines = nbuf[pl.ds(g * BLOCK, BLOCK)]
        part = pl.ds(g * BLOCK, BLOCK)

        def up_cols(col, width):
            weights = gu_all[:, :, col : col + width].reshape(NZ * NY * 64, width)
            return jnp.dot(lines, weights, preferred_element_type=F32)

        for col in (0, 256):
            hidden = silu(up_cols(col, 256)) * up_cols(768 + col, 256)
            hbuf[part, col : col + 256] = hidden.astype(BF16)
        tail = up_cols(512, 256)
        hidden = silu(tail[:, :128]) * up_cols(1280, 128)
        hbuf[part, 512:640] = hidden.astype(BF16)
        mixed_tile = tail[:, 128:]
        hidden = silu(mixed_tile) * pltpu.roll(mixed_tile, 64, 1)
        lane = lax.broadcasted_iota(jnp.int32, hidden.shape, 1)
        hbuf[part, 640:768] = jnp.where(lane < 64, hidden, 0.0).astype(BF16)

    def down_block(g):
        def term(j, core):
            weights = dn_all[pl.ds((2 * j + core) * 4, 4)].reshape(256, dn_all.shape[2])
            return lax.dot_general(
                hbuf[pl.ds(g * BLOCK, BLOCK)], weights, (((1,), (1,)), ((), ())),
                preferred_element_type=F32,
            )

        place(1, g, term)

    def mixed_chunk(i):
        summed = sbuf[i, c, x].astype(F32) + 0.5 * total(1, i)
        part = pl.ds(i * chunk, chunk)
        out_ref[part] = summed.astype(BF16)
        stores.append(pltpu.make_async_copy(out_ref.at[part], out_hbm.at[part], osem.at[i]))
        stores[-1].start()

    run(
        (
            (0, some_gated), (1, join_first), (2, relay_first),
            (3, stream_chunk), (4, spread_chunk), (5, far_chunk), (6, normed_chunk),
        ),
        pump,
    )

    dn_wait()
    down_block(0)
    down_block(1)

    def feed(tick):
        if tick == 0:
            up_block(2)
        elif tick == 1:
            down_block(2)
        elif tick == 2:
            up_block(3)
        elif tick == 3:
            down_block(3)

    def join_last(i):
        swap_join(1, i)

    def relay_last(i):
        relay(1, i)

    run(((0, join_last), (2, relay_last), (4, mixed_chunk)), feed)

    def drain():
        for copy in stores:
            copy.wait()
        for group in (*sums_out, gather_out):
            left(sbuf.at[pl.ds(0, 7)], group)
        left(gu_all.at[pl.ds(0, 31), pl.ds(0, gu_rows)], gu_out)
        left(gu_all.at[pl.ds(0, 31), pl.ds(0, gu_rows)], low_out)
        left(dn_all.at[pl.ds(0, 31)], dn_out)
        left(s1_buf.at[pl.ds(0, NY - 1)], s1_out)
        left(s3_buf.at[pl.ds(0, NY - 1)], s3_out)
        for d in range(1, NZ):

            @pl.when(z + d < NZ)
            def _(d=d):
                state_copy(d).wait_send()

    drain()
    assert slots.used <= RECEIVES, slots.used


RECEIVES, SENDS = 140, 15


def local(
    queries,
    cell_key_rows,
    cell_value_rows,
    output_gate_logits,
    input_gate_logits,
    forget_gate_logits,
    forget_extra_term,
    residual,
    head_norm_gain,
    cell_output_weight,
    feedforward_norm_gain,
    gate_projection_weight,
    up_projection_weight,
    down_projection_weight,
):
    rows = queries.shape[0]
    chunk = rows // CHUNKS
    half = chunk // 2
    vmem = pltpu.VMEM
    arguments = (
        queries,
        cell_key_rows,
        cell_value_rows,
        output_gate_logits,
        input_gate_logits,
        forget_gate_logits,
        forget_extra_term,
        residual,
        head_norm_gain,
        cell_output_weight,
        feedforward_norm_gain,
        gate_projection_weight,
        up_projection_weight,
        down_projection_weight.T,
    )
    scratch = [vmem(a.shape, a.dtype) for a in arguments] + [
        vmem(residual.shape, BF16),
        vmem((NZ * NY, 64, 1408), BF16),
        vmem((NZ * NY, 64, 768), BF16),
        vmem((NY, 48, 256), BF16),
        vmem((NY, 48, 256), BF16),
        vmem((1, 48, 256), BF16),
        vmem((NZ, 48, 256), BF16),
        vmem((NY, 48, 256), BF16),
        vmem((NY, 48, 256), BF16),
        vmem((128, 256), BF16),
        vmem((rows, 256), F32),
        vmem((2, CHUNKS, 2, NX, chunk, 256), BF16),
        vmem((2, CHUNKS, NX, chunk, 256), BF16),
        vmem((2, CHUNKS, NX, chunk, 256), BF16),
        vmem((2, CHUNKS, 2, half, 256), BF16),
        vmem((2, CHUNKS, 2, half, 256), BF16),
        vmem((2, CHUNKS, 2, 2, half, 256), BF16),
        vmem((CHUNKS, 2, NX, chunk, 256), BF16),
        vmem((rows, 2048), BF16),
        vmem((rows, 768), BF16),
        pltpu.SemaphoreType.DMA((SENDS,)),
        pltpu.SemaphoreType.DMA((RECEIVES,)),
        pltpu.SemaphoreType.DMA((len(arguments),)),
        pltpu.SemaphoreType.DMA((CHUNKS,)),
    ]
    return pl.pallas_call(
        cell_kernel,
        out_shape=jax.ShapeDtypeStruct(residual.shape, BF16),
        in_specs=[pl.BlockSpec(memory_space=pl.ANY)] * 14,
        out_specs=pl.BlockSpec(memory_space=pl.ANY),
        scratch_shapes=scratch,
        compiler_params=pltpu.CompilerParams(
            collective_id=0, has_side_effects=True, vmem_limit_bytes=62 * 1024 * 1024
        ),
    )(*arguments)


def solution(mesh):
    torus = Mesh(mesh.devices.reshape(NZ, NY, NX, 2), ("z", "y", "x", "c"))
    seq, head = ("z", "y"), ("x", "c")
    in_specs = (
        P(seq, head),
        P(seq, head),
        P(seq, head),
        P(seq, head),
        P(head, seq),
        P(head, seq),
        P(head, seq),
        P(seq, head),
        P(head),
        P(head, None),
        P(),
        P(seq, head),
        P(seq, head),
        P(head, seq),
    )
    return jax.shard_map(
        local, mesh=torus, in_specs=in_specs, out_specs=P(seq, head), check_vma=False
    )
```

```python
import jax
import jax.numpy as jnp
from jax import lax
from jax.experimental import pallas as pl
from jax.experimental.pallas import tpu as pltpu
from jax.sharding import Mesh
from jax.sharding import PartitionSpec as P

MESH = pl.DeviceIdType.MESH
F32 = jnp.float32
BF16 = jnp.bfloat16
LOWEST_LOG = -1e30
EPSILON = 1e-06
NZ, NY, NX = 8, 4, 4
CHUNKS = 8
BLOCKS = 4
PER_BLOCK = CHUNKS // BLOCKS
BLOCK = 256
EARLY = ((0, 1), (0, 1, 2, 3, 4, 7))


class Slots:
    def __init__(self):
        self.used = 0

    def take(self, count=1):
        first = self.used
        self.used += count
        return first


def running_rows(row, combine, identity):
    length = row.shape[1]
    lane = lax.broadcasted_iota(jnp.int32, row.shape, 1)
    step = 1
    while step < length:
        moved = jnp.where(lane >= step, pltpu.roll(row, step, 1), identity)
        row = combine(row, moved)
        step *= 2
    return row


def as_columns(row):
    return jnp.broadcast_to(row, (128, row.shape[1])).T


def wide(tile, copies):
    return jnp.concatenate([tile] * copies, axis=1)


def join(early, late):
    state_early, top_early, total_early = early
    state_late, top_late, total_late = late
    moved = top_early + total_late
    top = jnp.maximum(moved, top_late)
    left = wide(jnp.exp(moved - top), 2)
    right = wide(jnp.exp(top_late - top), 2)
    return (left * state_early + right * state_late, top, total_early + total_late)


def in_three(value):
    high = value.astype(BF16).astype(F32)
    middle = (value - high).astype(BF16).astype(F32)
    low = value - high - middle
    at = lax.broadcasted_iota(jnp.int32, (16, 128), 0)
    tile = jnp.where(at == 0, high, jnp.where(at == 1, middle, jnp.where(at == 2, low, 0.0)))
    return tile.astype(BF16)


def load_triple(ref, index):
    part = ref[index].astype(F32)
    scalars = part[32:33] + part[33:34] + part[34:35]
    return (part[0:32], scalars[:, 0:128], scalars[:, 128:256])


def store_triple(ref, index, triple):
    state, top, total = triple
    ref[index, 0:32, :] = state.astype(BF16)
    ref[index, 32:48, 0:128] = in_three(top)
    ref[index, 32:48, 128:256] = in_three(total)


def cell_kernel(
    q_in, k_in, v_in, og_in, ig_in, fg_in, ex_in, res_in, hg_in, wo_in, ng_in,
    gate_in, up_in, down_in,
    out_hbm,
    q_ref, k_ref, v_ref, og_ref, ig_ref, fg_ref, ex_ref, res_ref, hg_ref, wo_ref, ng_ref,
    gate_ref, up_ref, down_ref, out_ref,
    gu_all, dn_all, s1_src, s1_buf, s2_src, s2_buf, s3_src, s3_buf, state_ref,
    num_ref, pbuf, prcv, qbuf, rly, rsum, fin, sbuf, nbuf, hbuf,
    ssem, rsem, isem, osem,
):
    z, y, x, c = (lax.axis_index(a) for a in ("z", "y", "x", "c"))
    rows = q_ref.shape[0]
    chunk = rows // CHUNKS
    half = chunk // 2
    other = 1 - c
    x_at = [lax.rem(x + d, NX) for d in range(NX)]
    y_at = [lax.rem(y + d, NY) for d in range(NY)]
    z_at = [lax.rem(z + d, NZ) for d in range(NZ)]
    to_right, to_left, to_mate = {"x": x_at[1]}, {"x": x_at[3]}, {"c": other}
    y_right, y_left = {"y": y_at[1]}, {"y": y_at[3]}
    z_right, z_left = {"z": z_at[1]}, {"z": z_at[7]}
    stores, slots = [], Slots()

    def remote(src, dst, group, number, device):
        return pltpu.make_async_remote_copy(
            src_ref=src, dst_ref=dst, send_sem=ssem.at[group], recv_sem=rsem.at[number],
            device_id=device, device_id_type=MESH,
        )

    def send(src, dst, number, device, group):
        remote(src, dst, group, number, device).start()

    def arrived(dst, number):
        remote(dst, dst, 0, number, to_mate).wait_recv()

    def left(src, group):
        remote(src, src, group, 0, to_mate).wait_send()

    sums_out, gather_out, gu_out, dn_out, s1_out, s3_out, low_out, s2_out = (0, 1), 2, 3, 4, 5, 6, 7, 8

    own = z * NY + y

    loads = {}
    for number, (name, src, dst) in enumerate((
        ("gate", gate_in, gate_ref), ("up", up_in, up_ref), ("down", down_in, down_ref),
        ("ig", ig_in, ig_ref), ("fg", fg_in, fg_ref), ("ex", ex_in, ex_ref),
        ("k", k_in, k_ref), ("v", v_in, v_ref), ("q", q_in, q_ref),
        ("hg", hg_in, hg_ref), ("ng", ng_in, ng_ref), ("og", og_in, og_ref),
        ("wo", wo_in, wo_ref), ("res", res_in, res_ref),
    )):
        loads[name] = pltpu.make_async_copy(src, dst, isem.at[number])

    def loaded(*names):
        for name in names:
            loads[name].wait()

    def enter():
        low = jnp.full((1, 128), LOWEST_LOG, F32)
        for j in range(NZ):
            store_triple(s2_buf, j, (jnp.zeros((32, 256), F32), low, jnp.zeros((1, 128), F32)))
        for copy in loads.values():
            copy.start()
        for device in partners:
            pl.semaphore_signal(barrier, inc=1, device_id=device, device_id_type=MESH)

    def lay_weights():
        loaded("gate", "up", "down")
        gate, up, down = gate_ref[...], up_ref[...], down_ref[...]
        gu_all[own, :, 0:640] = gate[:, 0:640]
        gu_all[own, :, 640:768] = jnp.concatenate([gate[:, 640:704], up[:, 640:704]], axis=1)
        gu_all[own, :, 768:1408] = up[:, 0:640]
        dn_all[own, :, 0:640] = down[:, 0:640]
        dn_all[own, :, 640:768] = jnp.concatenate(
            [down[:, 640:704], jnp.zeros((64, 64), BF16)], axis=1
        )

    barrier = pltpu.get_barrier_semaphore()
    partners = [to_right, to_left, to_mate]
    partners += [{"y": y_at[d]} for d in range(1, NY)] + [{"z": z_at[d]} for d in range(1, NZ)]

    def meet():
        pl.semaphore_wait(barrier, len(partners))

    z_order = [0, 7, 1, 6, 2, 5, 3, 4]

    class ZFirst:
        def __init__(self, ref, count, group):
            self.ref, self.count, self.group = ref, count, group
            self.along_z, self.along_y, self.far = slots.take(4), slots.take(NZ), slots.take()

        def part(self, block, first, count):
            return self.ref.at[block, pl.ds(first, count)]

        def pass_on(self, at, number, device):
            send(at, at, number, device, self.group)

        def taken(self, blocks, number):
            arrived(self.ref.at[pl.ds(0, blocks), pl.ds(0, self.count)], number)

        def z_send(self, step):
            half_rows = self.count // 2
            for d, first, device in (((NZ - step) % NZ, 0, z_right), (step, half_rows, z_left)):
                block = z_at[d] * NY + y
                whole = (0, self.count) if step < 3 else (first, half_rows)
                self.pass_on(self.part(block, *whole), self.along_z + step, device)

        def z_wait(self, step):
            self.taken(2 if step < 3 else 1, self.along_z + step)

        def y_send(self, k):
            at = self.part(z_at[z_order[k]] * NY + y, 0, self.count)
            self.pass_on(at, self.along_y + k, y_right)
            self.pass_on(at, self.along_y + k, y_left)

        def y_forward(self, k):
            self.taken(2, self.along_y + k)
            block, half_rows = z_at[z_order[k]] * NY, self.count // 2
            self.pass_on(self.part(block + y_at[3], 0, half_rows), self.far, y_right)
            self.pass_on(self.part(block + y_at[1], half_rows, half_rows), self.far, y_left)

        def y_wait(self):
            self.taken(NZ, self.far)

    class YFirst:
        def __init__(self, ref, first, count, group):
            self.ref, self.first, self.count, self.group = ref, first, count, group
            self.along_y, self.far, self.along_z = slots.take(), slots.take(), slots.take(7)

        def pass_on(self, at, number, device):
            send(at, at, number, device, self.group)

        def taken(self, blocks, number):
            arrived(self.ref.at[pl.ds(0, blocks), pl.ds(self.first, self.count)], number)

        def y_send(self):
            at = self.ref.at[own, pl.ds(self.first, self.count)]
            self.pass_on(at, self.along_y, y_right)
            self.pass_on(at, self.along_y, y_left)

        def y_forward(self):
            self.taken(2, self.along_y)
            half_rows = self.count // 2
            at = self.ref.at[z * NY + y_at[3], pl.ds(self.first, half_rows)]
            self.pass_on(at, self.far, y_right)
            at = self.ref.at[z * NY + y_at[1], pl.ds(self.first + half_rows, half_rows)]
            self.pass_on(at, self.far, y_left)

        def y_wait(self):
            self.taken(1, self.far)

        def pair(self, d, part):
            return self.ref.at[pl.ds(z_at[d] * NY + 2 * part, 2), pl.ds(self.first, self.count)]

        def z_send(self, step, part):
            if step < 3:
                number = self.along_z + 2 * step + part
                self.pass_on(self.pair((NZ - step) % NZ, part), number, z_right)
                self.pass_on(self.pair(step, part), number, z_left)
            elif part == 0:
                self.pass_on(self.pair(5, 0), self.along_z + 6, z_right)
            else:
                self.pass_on(self.pair(3, 1), self.along_z + 6, z_left)

        def z_wait(self, step, part):
            self.taken(4, self.along_z + 2 * step + part)

    gu_rows = gu_all.shape[1] // 2
    top_gu = ZFirst(gu_all, gu_rows, gu_out)
    low_gu = YFirst(gu_all, gu_rows, gu_rows, low_out)
    dn = ZFirst(dn_all, dn_all.shape[1], dn_out)

    def gates():
        loaded("ig", "fg", "ex")
        logits = fg_ref[...].astype(F32)
        log_forget = jnp.minimum(logits, 0.0) - jnp.log1p(jnp.exp(-jnp.abs(logits))) + ex_ref[...]
        cum = running_rows(log_forget, jnp.add, 0.0)
        lead = ig_ref[...].astype(F32) - cum
        return cum, lead, running_rows(lead, jnp.maximum, -jnp.inf)

    s1, s2, s3 = slots.take(), slots.take(NZ - 1) - 1, slots.take()

    def end_parts():
        loaded("k", "v")
        last_cum, last_lead = cum[:, rows - 1 :], top_run[:, rows - 1 :]
        weight = as_columns(jnp.exp(lead - last_lead))
        scaled = (k_ref[...].astype(F32) * weight).astype(BF16)
        end_state = lax.dot_general(
            scaled, v_ref[...], (((0,), (0,)), ((), ())), preferred_element_type=F32
        )
        end_top = jnp.broadcast_to(last_cum + last_lead, (1, 128))
        end_total = jnp.broadcast_to(last_cum, (1, 128))
        for p in range(NY):
            store_triple(s1_src, p, (end_state[p * 32 : p * 32 + 32], end_top, end_total))
        s1_buf[y] = s1_src[y]

    def send_parts():
        for d in range(1, NY):
            send(s1_src.at[y_at[d]], s1_buf.at[y], s1, {"y": y_at[d]}, s1_out)

    step_rows = 256

    def local_rows(i):
        r0 = i * step_rows
        top_tile = top_cols[r0 : r0 + step_rows]
        parts = None
        for j in range(i + 1):
            s0 = j * step_rows
            scores = lax.dot_general(
                q_ref[r0 : r0 + step_rows], k_ref[s0 : s0 + step_rows],
                (((1,), (1,)), ((), ())), preferred_element_type=F32,
            )
            log_weight = lead[:, s0 : s0 + step_rows] - wide(top_tile, step_rows // 128)
            if i == j:
                at_row = lax.broadcasted_iota(jnp.int32, (step_rows, step_rows), 0)
                at_col = lax.broadcasted_iota(jnp.int32, (step_rows, step_rows), 1)
                log_weight = jnp.where(at_col <= at_row, log_weight, -jnp.inf)
            scores = (scores * (128.0**-0.5) * jnp.exp(log_weight)).astype(BF16)
            term = jnp.dot(scores, v_ref[s0 : s0 + step_rows], preferred_element_type=F32)
            parts = term if parts is None else parts + term
        num_ref[r0 : r0 + step_rows, :] = parts

    def state_copy(d):
        return remote(s2_src.at[0], s2_buf.at[z], s2_out + d - 1, s2 + d, {"z": z_at[d]})

    def y_states():
        arrived(s1_buf.at[pl.ds(0, NY - 1)], s1)
        inside = [load_triple(s1_buf, 0)]
        for j in range(1, NY):
            inside.append(join(inside[-1], load_triple(s1_buf, j)))
        store_triple(s2_src, 0, inside[-1])
        for d in range(1, NZ):

            @pl.when(z + d < NZ)
            def _(d=d):
                state_copy(d).start()

        return inside

    def z_states():
        for d in range(1, NZ):

            @pl.when(z - d >= 0)
            def _(d=d):
                arrived(s2_buf.at[z_at[NZ - d]], s2 + d)

        before = load_triple(s2_buf, 0)
        for j in range(1, NZ):
            before = join(before, load_triple(s2_buf, j))
        store_triple(s3_src, 0, before)
        for j in range(1, NY):
            store_triple(s3_src, j, join(before, inside[j - 1]))
        for d in range(1, NY):
            send(s3_src.at[y_at[d]], s3_buf.at[y], s3, {"y": y_at[d]}, s3_out)
        s3_buf[y] = s3_src[y]

    def carried():
        arrived(s3_buf.at[pl.ds(0, NY - 1)], s3)
        for p in range(NY):
            state_ref[p * 32 : p * 32 + 32, :] = s3_buf[p, 0:32, :]
        return load_triple(s3_buf, 0)[1]

    enter()
    lay_weights()
    cum, lead, top_run = gates()
    end_parts()
    meet()
    send_parts()
    top_gu.z_send(0)
    low_gu.y_send()
    top_gu.y_send(0)
    top_cols = as_columns(top_run)
    loaded("q", "hg", "ng", "og", "wo", "res")
    head_gain = hg_ref[...].astype(F32).reshape(1, 256)
    feed_gain = ng_ref[...].astype(F32).reshape(1, 2048)
    for i in range(4):
        local_rows(i)
    inside = y_states()
    top_gu.z_wait(0)
    top_gu.z_send(1)
    dn.z_send(0)
    top_gu.y_send(1)
    top_gu.y_send(2)
    z_states()
    low_gu.y_forward()
    top_gu.y_forward(0)
    dn.y_send(0)
    carried_top = carried()

    def reduce_slots():
        return [slots.take(4) for _ in range(CHUNKS)]

    sums = (reduce_slots(), reduce_slots())
    gathers = [slots.take(4) for _ in range(CHUNKS)]

    def swap_send(a, i):
        send(pbuf.at[a, i, other], prcv.at[a, i], sums[a][i], to_mate, sums_out[a])

    def swap_join(a, i):
        n = sums[a][i]
        arrived(prcv.at[a, i], n)
        for j in range(NX):
            both = pbuf[a, i, c, j].astype(F32) + prcv[a, i, j].astype(F32)
            qbuf[a, i, j] = both.astype(BF16)
        top, low = pl.ds(0, half), pl.ds(half, half)
        send(qbuf.at[a, i, x_at[2], top], rly.at[a, i, 0], n + 1, to_right, sums_out[a])
        send(qbuf.at[a, i, x_at[2], low], rly.at[a, i, 1], n + 2, to_left, sums_out[a])
        if i in EARLY[a]:
            direct(a, i)

    def direct(a, i):
        n = sums[a][i]
        top, low = pl.ds(0, half), pl.ds(half, half)
        send(qbuf.at[a, i, x_at[1], low], fin.at[a, i, 0, 1], n + 3, to_right, sums_out[a])
        send(qbuf.at[a, i, x_at[3], top], fin.at[a, i, 1, 0], n + 3, to_left, sums_out[a])

    def relay(a, i):
        n = sums[a][i]
        arrived(rly.at[a, i, 0], n + 1)
        added = rly[a, i, 0].astype(F32) + qbuf[a, i, x_at[1], 0:half].astype(F32)
        rsum[a, i, 0] = added.astype(BF16)
        send(rsum.at[a, i, 0], fin.at[a, i, 0, 0], n + 3, to_right, sums_out[a])
        arrived(rly.at[a, i, 1], n + 2)
        added = rly[a, i, 1].astype(F32) + qbuf[a, i, x_at[3], half:].astype(F32)
        rsum[a, i, 1] = added.astype(BF16)
        send(rsum.at[a, i, 1], fin.at[a, i, 1, 1], n + 3, to_left, sums_out[a])
        if i not in EARLY[a]:
            direct(a, i)

    def total(a, i):
        n = sums[a][i]
        arrived(fin.at[a, i], n + 3)
        found = []
        for h in range(2):
            own = qbuf[a, i, x, h * half : h * half + half].astype(F32)
            found.append(own + fin[a, i, 0, h].astype(F32) + fin[a, i, 1, h].astype(F32))
        return jnp.concatenate(found, axis=0)

    def gated_block(g):
        part = pl.ds(g * BLOCK, BLOCK)
        run = top_cols[g * BLOCK : g * BLOCK + BLOCK]
        top = jnp.maximum(run, carried_top)
        keep = wide(jnp.exp(run - top), 2)
        enter = wide(jnp.exp(carried_top - top) * (128.0**-0.5), 2)
        earlier = jnp.dot(q_ref[part], state_ref[...], preferred_element_type=F32)
        memory = keep * num_ref[part] + enter * earlier
        mean = jnp.mean(memory * memory, axis=1, keepdims=True)
        opened = jax.nn.sigmoid(og_ref[part].astype(F32))
        gated = memory * lax.rsqrt(mean + EPSILON) * head_gain * opened
        gated = gated.astype(BF16)
        def term(j, core):
            columns = pl.ds(pl.multiple_of((2 * j + core) * 256, 256), 256)
            return jnp.dot(gated, wo_ref[:, columns], preferred_element_type=F32)

        place(0, g, term)

    def place(a, g, term):
        for core in (other, c):
            for j in range(NX):
                found = term(j, core).astype(BF16)
                for i in range(PER_BLOCK):
                    pbuf[a, g * PER_BLOCK + i, core, j] = found[i * chunk : i * chunk + chunk]
            if core is other:
                for i in range(PER_BLOCK):
                    swap_send(a, g * PER_BLOCK + i)

    def stream_chunk(i):
        n = gathers[i]
        summed = total(0, i) + res_ref[pl.ds(i * chunk, chunk)].astype(F32)
        sbuf[i, c, x] = summed.astype(BF16)
        at = sbuf.at[i, c, x]
        send(at, at, n, to_right, gather_out)
        send(at, at, n + 1, to_left, gather_out)
        send(at, at, n + 3, to_mate, gather_out)

    def spread_chunk(i):
        n = gathers[i]
        for number, d, first, device in ((n, 3, 0, to_right), (n + 1, 1, half, to_left)):
            at = sbuf.at[i, c, x_at[d]]
            arrived(at, number)
            part = sbuf.at[i, c, x_at[d], pl.ds(first, half)]
            send(part, part, n + 2, device, gather_out)
            send(at, at, n + 3, to_mate, gather_out)

    def far_chunk(i):
        n = gathers[i]
        at = sbuf.at[i, c, x_at[2]]
        arrived(at, n + 2)
        send(at, at, n + 3, to_mate, gather_out)

    def normed_chunk(i):
        arrived(sbuf.at[i, other], gathers[i] + 3)
        square = jnp.zeros((chunk, 256), F32)
        for b in range(2 * NX):
            part = sbuf[i, b % 2, b // 2].astype(F32)
            square = square + part * part
        mean = jnp.sum(square, axis=1, keepdims=True) * (1.0 / (2 * NX * 256))
        scale = lax.rsqrt(mean + EPSILON)
        for b in range(2 * NX):
            cols = slice(b * 256, b * 256 + 256)
            part = sbuf[i, b % 2, b // 2].astype(F32)
            nbuf[pl.ds(i * chunk, chunk), cols] = (part * scale * feed_gain[:, cols]).astype(BF16)

    def pump(tick):
        if tick == 0:
            top_gu.z_wait(1)
            top_gu.z_send(2)
            low_gu.y_wait()
            low_gu.z_send(0, 0)
            top_gu.y_send(3)
            top_gu.y_send(4)
            dn.z_wait(0)
            dn.z_send(1)
            dn.y_send(1)
        elif tick == 1:
            low_gu.z_send(0, 1)
        elif tick == 2:
            top_gu.y_forward(1)
            dn.y_send(2)
        elif tick == 3:
            top_gu.z_wait(2)
            top_gu.z_send(3)
            top_gu.y_send(5)
            top_gu.y_send(6)
            top_gu.y_forward(2)
        elif tick == 4:
            dn.z_wait(1)
            dn.z_send(2)
            top_gu.y_forward(3)
            dn.y_send(3)
            low_gu.z_wait(0, 0)
            low_gu.z_send(1, 0)
        elif tick == 5:
            top_gu.z_wait(3)
            top_gu.y_send(7)
            top_gu.y_forward(4)
            dn.y_send(4)
            low_gu.z_wait(0, 1)
            low_gu.z_send(1, 1)
        elif tick == 6:
            dn.z_wait(2)
            dn.z_send(3)
            top_gu.y_forward(5)
            top_gu.y_forward(6)
            dn.y_forward(0)
            dn.y_send(5)
            low_gu.z_wait(1, 0)
            low_gu.z_send(2, 0)
        elif tick == 7:
            top_gu.y_forward(7)
            dn.y_send(6)
            dn.y_forward(1)
            dn.y_forward(2)
            low_gu.z_wait(1, 1)
            low_gu.z_send(2, 1)
        elif tick == 8:
            dn.z_wait(3)
            dn.y_send(7)
            dn.y_forward(3)
            low_gu.z_wait(2, 0)
            low_gu.z_send(3, 0)
        elif tick == 9:
            dn.y_forward(4)
            dn.y_forward(5)
            low_gu.z_wait(2, 1)
            low_gu.z_send(3, 1)
        elif tick == 10:
            dn.y_forward(6)
            dn.y_forward(7)
        elif tick == 11:
            gu_wait()
            up_block(0)
        elif tick == 12:
            dn_wait()
            down_block(0)

    def gu_wait():
        low_gu.taken(4, low_gu.along_z + 6)
        top_gu.y_wait()

    def dn_wait():
        dn.y_wait()

    def run(stages, pump=None):
        for tick in range(CHUNKS + max(lag for lag, _ in stages)):
            for lag, stage in stages:
                if 0 <= tick - lag < CHUNKS:
                    stage(tick - lag)
            if pump is not None:
                pump(tick)

    def join_first(i):
        swap_join(0, i)

    def relay_first(i):
        relay(0, i)

    def some_gated(i):
        if i < BLOCKS:
            gated_block(i)

    def silu(v):
        return v / (1.0 + jnp.exp(-v))

    def up_block(g):
        lines = nbuf[pl.ds(g * BLOCK, BLOCK)]
        part = pl.ds(g * BLOCK, BLOCK)

        def up_cols(col, width):
            weights = gu_all[:, :, col : col + width].reshape(NZ * NY * 64, width)
            return jnp.dot(lines, weights, preferred_element_type=F32)

        for col in (0, 256):
            hidden = silu(up_cols(col, 256)) * up_cols(768 + col, 256)
            hbuf[part, col : col + 256] = hidden.astype(BF16)
        tail = up_cols(512, 256)
        hidden = silu(tail[:, :128]) * up_cols(1280, 128)
        hbuf[part, 512:640] = hidden.astype(BF16)
        mixed_tile = tail[:, 128:]
        hidden = silu(mixed_tile) * pltpu.roll(mixed_tile, 64, 1)
        lane = lax.broadcasted_iota(jnp.int32, hidden.shape, 1)
        hbuf[part, 640:768] = jnp.where(lane < 64, hidden, 0.0).astype(BF16)

    def down_block(g):
        def term(j, core):
            weights = dn_all[pl.ds((2 * j + core) * 4, 4)].reshape(256, dn_all.shape[2])
            return lax.dot_general(
                hbuf[pl.ds(g * BLOCK, BLOCK)], weights, (((1,), (1,)), ((), ())),
                preferred_element_type=F32,
            )

        place(1, g, term)

    def mixed_chunk(i):
        summed = sbuf[i, c, x].astype(F32) + 0.5 * total(1, i)
        part = pl.ds(i * chunk, chunk)
        out_ref[part] = summed.astype(BF16)
        stores.append(pltpu.make_async_copy(out_ref.at[part], out_hbm.at[part], osem.at[i]))
        stores[-1].start()

    run(
        (
            (0, some_gated), (1, join_first), (2, relay_first),
            (3, stream_chunk), (4, spread_chunk), (5, far_chunk), (6, normed_chunk),
        ),
        pump,
    )

    def drain():
        left(sbuf.at[pl.ds(0, 7)], sums_out[0])
        left(sbuf.at[pl.ds(0, 7)], gather_out)
        left(gu_all.at[pl.ds(0, 31), pl.ds(0, gu_rows)], gu_out)
        left(gu_all.at[pl.ds(0, 31), pl.ds(0, gu_rows)], low_out)
        left(dn_all.at[pl.ds(0, 31)], dn_out)
        left(s1_buf.at[pl.ds(0, NY - 1)], s1_out)
        left(s3_buf.at[pl.ds(0, NY - 1)], s3_out)
        for d in range(1, NZ):

            @pl.when(z + d < NZ)
            def _(d=d):
                state_copy(d).wait_send()

    def last(*steps):
        for name, at in steps:
            if name == "up":
                up_block(at)
            elif name == "down":
                down_block(at)
            elif name == "join":
                swap_join(1, at)
            elif name == "relay":
                relay(1, at)
            else:
                mixed_chunk(at)

    last(
        ("join", 0), ("up", 1), ("join", 1), ("down", 1), ("relay", 0), ("up", 2),
        ("join", 2), ("relay", 1), ("down", 2), ("join", 3), ("up", 3), ("join", 4),
        ("relay", 2), ("mixed", 0), ("down", 3), ("join", 5), ("relay", 3), ("mixed", 1),
        ("join", 6), ("relay", 4), ("mixed", 2), ("join", 7), ("relay", 5), ("mixed", 3),
        ("relay", 6), ("mixed", 4), ("relay", 7), ("mixed", 5), ("mixed", 6),
    )
    drain()
    mixed_chunk(7)
    for copy in stores:
        copy.wait()
    left(sbuf.at[pl.ds(0, 7)], sums_out[1])
    assert slots.used <= RECEIVES, slots.used


RECEIVES, SENDS = 140, 15


def local(
    queries,
    cell_key_rows,
    cell_value_rows,
    output_gate_logits,
    input_gate_logits,
    forget_gate_logits,
    forget_extra_term,
    residual,
    head_norm_gain,
    cell_output_weight,
    feedforward_norm_gain,
    gate_projection_weight,
    up_projection_weight,
    down_projection_weight,
):
    rows = queries.shape[0]
    chunk = rows // CHUNKS
    half = chunk // 2
    vmem = pltpu.VMEM
    arguments = (
        queries,
        cell_key_rows,
        cell_value_rows,
        output_gate_logits,
        input_gate_logits,
        forget_gate_logits,
        forget_extra_term,
        residual,
        head_norm_gain,
        cell_output_weight,
        feedforward_norm_gain,
        gate_projection_weight,
        up_projection_weight,
        down_projection_weight.T,
    )
    scratch = [vmem(a.shape, a.dtype) for a in arguments] + [
        vmem(residual.shape, BF16),
        vmem((NZ * NY, 64, 1408), BF16),
        vmem((NZ * NY, 64, 768), BF16),
        vmem((NY, 48, 256), BF16),
        vmem((NY, 48, 256), BF16),
        vmem((1, 48, 256), BF16),
        vmem((NZ, 48, 256), BF16),
        vmem((NY, 48, 256), BF16),
        vmem((NY, 48, 256), BF16),
        vmem((128, 256), BF16),
        vmem((rows, 256), F32),
        vmem((2, CHUNKS, 2, NX, chunk, 256), BF16),
        vmem((2, CHUNKS, NX, chunk, 256), BF16),
        vmem((2, CHUNKS, NX, chunk, 256), BF16),
        vmem((2, CHUNKS, 2, half, 256), BF16),
        vmem((2, CHUNKS, 2, half, 256), BF16),
        vmem((2, CHUNKS, 2, 2, half, 256), BF16),
        vmem((CHUNKS, 2, NX, chunk, 256), BF16),
        vmem((rows, 2048), BF16),
        vmem((rows, 768), BF16),
        pltpu.SemaphoreType.DMA((SENDS,)),
        pltpu.SemaphoreType.DMA((RECEIVES,)),
        pltpu.SemaphoreType.DMA((len(arguments),)),
        pltpu.SemaphoreType.DMA((CHUNKS,)),
    ]
    return pl.pallas_call(
        cell_kernel,
        out_shape=jax.ShapeDtypeStruct(residual.shape, BF16),
        in_specs=[pl.BlockSpec(memory_space=pl.ANY)] * 14,
        out_specs=pl.BlockSpec(memory_space=pl.ANY),
        scratch_shapes=scratch,
        compiler_params=pltpu.CompilerParams(
            collective_id=0, has_side_effects=True, vmem_limit_bytes=62 * 1024 * 1024
        ),
    )(*arguments)


def solution(mesh):
    torus = Mesh(mesh.devices.reshape(NZ, NY, NX, 2), ("z", "y", "x", "c"))
    seq, head = ("z", "y"), ("x", "c")
    in_specs = (
        P(seq, head),
        P(seq, head),
        P(seq, head),
        P(seq, head),
        P(head, seq),
        P(head, seq),
        P(head, seq),
        P(seq, head),
        P(head),
        P(head, None),
        P(),
        P(seq, head),
        P(seq, head),
        P(head, seq),
    )
    return jax.shard_map(
        local, mesh=torus, in_specs=in_specs, out_specs=P(seq, head), check_vma=False
    )
```

```python
import jax
import jax.numpy as jnp
from jax import lax
from jax.experimental import pallas as pl
from jax.experimental.pallas import tpu as pltpu
from jax.sharding import Mesh
from jax.sharding import PartitionSpec as P

MESH = pl.DeviceIdType.MESH
F32 = jnp.float32
BF16 = jnp.bfloat16
LOWEST_LOG = -1e30
EPSILON = 1e-06
NZ, NY, NX = 8, 4, 4
CHUNKS = 8
BLOCKS = 4
PER_BLOCK = CHUNKS // BLOCKS
BLOCK = 256
EARLY = ((0, 1), (0, 1, 2, 3, 4, 7))


class Slots:
    def __init__(self):
        self.used = 0

    def take(self, count=1):
        first = self.used
        self.used += count
        return first


def running_rows(row, combine, identity):
    length = row.shape[1]
    lane = lax.broadcasted_iota(jnp.int32, row.shape, 1)
    step = 1
    while step < length:
        moved = jnp.where(lane >= step, pltpu.roll(row, step, 1), identity)
        row = combine(row, moved)
        step *= 2
    return row


def as_columns(row):
    return jnp.broadcast_to(row, (128, row.shape[1])).T


def wide(tile, copies):
    return jnp.concatenate([tile] * copies, axis=1)


def join(early, late):
    state_early, top_early, total_early = early
    state_late, top_late, total_late = late
    moved = top_early + total_late
    top = jnp.maximum(moved, top_late)
    left = wide(jnp.exp(moved - top), 2)
    right = wide(jnp.exp(top_late - top), 2)
    return (left * state_early + right * state_late, top, total_early + total_late)


def in_three(value):
    high = value.astype(BF16).astype(F32)
    middle = (value - high).astype(BF16).astype(F32)
    low = value - high - middle
    at = lax.broadcasted_iota(jnp.int32, (16, 128), 0)
    tile = jnp.where(at == 0, high, jnp.where(at == 1, middle, jnp.where(at == 2, low, 0.0)))
    return tile.astype(BF16)


def load_triple(ref, index):
    part = ref[index].astype(F32)
    scalars = part[32:33] + part[33:34] + part[34:35]
    return (part[0:32], scalars[:, 0:128], scalars[:, 128:256])


def store_triple(ref, index, triple):
    state, top, total = triple
    ref[index, 0:32, :] = state.astype(BF16)
    ref[index, 32:48, 0:128] = in_three(top)
    ref[index, 32:48, 128:256] = in_three(total)


def cell_kernel(
    q_in, k_in, v_in, og_in, ig_in, fg_in, ex_in, res_in, hg_in, wo_in, ng_in,
    gate_in, up_in, down_in,
    out_hbm,
    q_ref, k_ref, v_ref, og_ref, ig_ref, fg_ref, ex_ref, res_ref, hg_ref, wo_ref, ng_ref,
    gate_ref, up_ref, down_ref, out_ref,
    gu_all, dn_all, s1_src, s1_buf, s2_src, s2_buf, s3_src, s3_buf, state_ref,
    num_ref, pbuf, prcv, qbuf, rly, rsum, fin, sbuf, nbuf, hbuf,
    ssem, rsem, isem, osem,
):
    z, y, x, c = (lax.axis_index(a) for a in ("z", "y", "x", "c"))
    rows = q_ref.shape[0]
    chunk = rows // CHUNKS
    half = chunk // 2
    other = 1 - c
    x_at = [lax.rem(x + d, NX) for d in range(NX)]
    y_at = [lax.rem(y + d, NY) for d in range(NY)]
    z_at = [lax.rem(z + d, NZ) for d in range(NZ)]
    to_right, to_left, to_mate = {"x": x_at[1]}, {"x": x_at[3]}, {"c": other}
    y_right, y_left = {"y": y_at[1]}, {"y": y_at[3]}
    z_right, z_left = {"z": z_at[1]}, {"z": z_at[7]}
    stores, slots = [], Slots()

    def remote(src, dst, group, number, device):
        return pltpu.make_async_remote_copy(
            src_ref=src, dst_ref=dst, send_sem=ssem.at[group], recv_sem=rsem.at[number],
            device_id=device, device_id_type=MESH,
        )

    def send(src, dst, number, device, group):
        remote(src, dst, group, number, device).start()

    def arrived(dst, number):
        remote(dst, dst, 0, number, to_mate).wait_recv()

    def left(src, group):
        remote(src, src, group, 0, to_mate).wait_send()

    sums_out, gather_out, gu_out, dn_out, s1_out, s3_out, low_out, s2_out = (0, 1), 2, 3, 4, 5, 6, 7, 8

    own = z * NY + y

    loads = {}
    for number, (name, src, dst) in enumerate((
        ("gate", gate_in, gate_ref), ("up", up_in, up_ref), ("down", down_in, down_ref),
        ("ig", ig_in, ig_ref), ("fg", fg_in, fg_ref), ("ex", ex_in, ex_ref),
        ("k", k_in, k_ref), ("v", v_in, v_ref), ("q", q_in, q_ref),
        ("hg", hg_in, hg_ref), ("ng", ng_in, ng_ref), ("og", og_in, og_ref),
        ("wo", wo_in, wo_ref), ("res", res_in, res_ref),
    )):
        loads[name] = pltpu.make_async_copy(src, dst, isem.at[number])

    def loaded(*names):
        for name in names:
            loads[name].wait()

    def enter():
        low = jnp.full((1, 128), LOWEST_LOG, F32)
        for j in range(NZ):
            store_triple(s2_buf, j, (jnp.zeros((32, 256), F32), low, jnp.zeros((1, 128), F32)))
        for copy in loads.values():
            copy.start()
        for device in partners:
            pl.semaphore_signal(barrier, inc=1, device_id=device, device_id_type=MESH)

    def lay_weights():
        loaded("gate", "up", "down")
        gate, up, down = gate_ref[...], up_ref[...], down_ref[...]
        gu_all[own, :, 0:640] = gate[:, 0:640]
        gu_all[own, :, 640:768] = jnp.concatenate([gate[:, 640:704], up[:, 640:704]], axis=1)
        gu_all[own, :, 768:1408] = up[:, 0:640]
        dn_all[own, :, 0:640] = down[:, 0:640]
        dn_all[own, :, 640:768] = jnp.concatenate(
            [down[:, 640:704], jnp.zeros((64, 64), BF16)], axis=1
        )

    barrier = pltpu.get_barrier_semaphore()
    partners = [to_right, to_left, to_mate]
    partners += [{"y": y_at[d]} for d in range(1, NY)] + [{"z": z_at[d]} for d in range(1, NZ)]

    def meet():
        pl.semaphore_wait(barrier, len(partners))

    z_order = [0, 7, 1, 6, 2, 5, 3, 4]

    class ZFirst:
        def __init__(self, ref, count, group):
            self.ref, self.count, self.group = ref, count, group
            self.along_z, self.along_y, self.far = slots.take(4), slots.take(NZ), slots.take()

        def part(self, block, first, count):
            return self.ref.at[block, pl.ds(first, count)]

        def pass_on(self, at, number, device):
            send(at, at, number, device, self.group)

        def taken(self, blocks, number):
            arrived(self.ref.at[pl.ds(0, blocks), pl.ds(0, self.count)], number)

        def z_send(self, step):
            half_rows = self.count // 2
            for d, first, device in (((NZ - step) % NZ, 0, z_right), (step, half_rows, z_left)):
                block = z_at[d] * NY + y
                whole = (0, self.count) if step < 3 else (first, half_rows)
                self.pass_on(self.part(block, *whole), self.along_z + step, device)

        def z_wait(self, step):
            self.taken(2 if step < 3 else 1, self.along_z + step)

        def y_send(self, k):
            at = self.part(z_at[z_order[k]] * NY + y, 0, self.count)
            self.pass_on(at, self.along_y + k, y_right)
            self.pass_on(at, self.along_y + k, y_left)

        def y_forward(self, k):
            self.taken(2, self.along_y + k)
            block, half_rows = z_at[z_order[k]] * NY, self.count // 2
            self.pass_on(self.part(block + y_at[3], 0, half_rows), self.far, y_right)
            self.pass_on(self.part(block + y_at[1], half_rows, half_rows), self.far, y_left)

        def y_wait(self):
            self.taken(NZ, self.far)

    class YFirst:
        def __init__(self, ref, first, count, group):
            self.ref, self.first, self.count, self.group = ref, first, count, group
            self.along_y, self.far, self.along_z = slots.take(), slots.take(), slots.take(7)

        def pass_on(self, at, number, device):
            send(at, at, number, device, self.group)

        def taken(self, blocks, number):
            arrived(self.ref.at[pl.ds(0, blocks), pl.ds(self.first, self.count)], number)

        def y_send(self):
            at = self.ref.at[own, pl.ds(self.first, self.count)]
            self.pass_on(at, self.along_y, y_right)
            self.pass_on(at, self.along_y, y_left)

        def y_forward(self):
            self.taken(2, self.along_y)
            half_rows = self.count // 2
            at = self.ref.at[z * NY + y_at[3], pl.ds(self.first, half_rows)]
            self.pass_on(at, self.far, y_right)
            at = self.ref.at[z * NY + y_at[1], pl.ds(self.first + half_rows, half_rows)]
            self.pass_on(at, self.far, y_left)

        def y_wait(self):
            self.taken(1, self.far)

        def pair(self, d, part):
            return self.ref.at[pl.ds(z_at[d] * NY + 2 * part, 2), pl.ds(self.first, self.count)]

        def z_send(self, step, part):
            if step < 3:
                number = self.along_z + 2 * step + part
                self.pass_on(self.pair((NZ - step) % NZ, part), number, z_right)
                self.pass_on(self.pair(step, part), number, z_left)
            elif part == 0:
                self.pass_on(self.pair(5, 0), self.along_z + 6, z_right)
            else:
                self.pass_on(self.pair(3, 1), self.along_z + 6, z_left)

        def z_wait(self, step, part):
            self.taken(4, self.along_z + 2 * step + part)

    gu_rows = gu_all.shape[1] // 2
    top_gu = ZFirst(gu_all, gu_rows, gu_out)
    low_gu = YFirst(gu_all, gu_rows, gu_rows, low_out)
    dn = ZFirst(dn_all, dn_all.shape[1], dn_out)

    def gates():
        loaded("ig", "fg", "ex")
        logits = fg_ref[...].astype(F32)
        log_forget = jnp.minimum(logits, 0.0) - jnp.log1p(jnp.exp(-jnp.abs(logits))) + ex_ref[...]
        cum = running_rows(log_forget, jnp.add, 0.0)
        lead = ig_ref[...].astype(F32) - cum
        return cum, lead, running_rows(lead, jnp.maximum, -jnp.inf)

    s1, s2, s3 = slots.take(), slots.take(NZ - 1) - 1, slots.take()

    def end_parts():
        loaded("k", "v")
        last_cum, last_lead = cum[:, rows - 1 :], top_run[:, rows - 1 :]
        weight = as_columns(jnp.exp(lead - last_lead))
        scaled = (k_ref[...].astype(F32) * weight).astype(BF16)
        end_state = lax.dot_general(
            scaled, v_ref[...], (((0,), (0,)), ((), ())), preferred_element_type=F32
        )
        end_top = jnp.broadcast_to(last_cum + last_lead, (1, 128))
        end_total = jnp.broadcast_to(last_cum, (1, 128))
        for p in range(NY):
            store_triple(s1_src, p, (end_state[p * 32 : p * 32 + 32], end_top, end_total))
        s1_buf[y] = s1_src[y]

    def send_parts():
        for d in range(1, NY):
            send(s1_src.at[y_at[d]], s1_buf.at[y], s1, {"y": y_at[d]}, s1_out)

    step_rows = 256

    def local_rows(i):
        r0 = i * step_rows
        top_tile = top_cols[r0 : r0 + step_rows]
        parts = None
        for j in range(i + 1):
            s0 = j * step_rows
            scores = lax.dot_general(
                q_ref[r0 : r0 + step_rows], k_ref[s0 : s0 + step_rows],
                (((1,), (1,)), ((), ())), preferred_element_type=F32,
            )
            log_weight = lead[:, s0 : s0 + step_rows] - wide(top_tile, step_rows // 128)
            if i == j:
                at_row = lax.broadcasted_iota(jnp.int32, (step_rows, step_rows), 0)
                at_col = lax.broadcasted_iota(jnp.int32, (step_rows, step_rows), 1)
                log_weight = jnp.where(at_col <= at_row, log_weight, -jnp.inf)
            scores = (scores * (128.0**-0.5) * jnp.exp(log_weight)).astype(BF16)
            term = jnp.dot(scores, v_ref[s0 : s0 + step_rows], preferred_element_type=F32)
            parts = term if parts is None else parts + term
        num_ref[r0 : r0 + step_rows, :] = parts

    def state_copy(d):
        return remote(s2_src.at[0], s2_buf.at[z], s2_out + d - 1, s2 + d, {"z": z_at[d]})

    def y_states():
        arrived(s1_buf.at[pl.ds(0, NY - 1)], s1)
        inside = [load_triple(s1_buf, 0)]
        for j in range(1, NY):
            inside.append(join(inside[-1], load_triple(s1_buf, j)))
        store_triple(s2_src, 0, inside[-1])
        for d in range(1, NZ):

            @pl.when(z + d < NZ)
            def _(d=d):
                state_copy(d).start()

        return inside

    def z_states():
        for d in range(1, NZ):

            @pl.when(z - d >= 0)
            def _(d=d):
                arrived(s2_buf.at[z_at[NZ - d]], s2 + d)

        before = load_triple(s2_buf, 0)
        for j in range(1, NZ):
            before = join(before, load_triple(s2_buf, j))
        store_triple(s3_src, 0, before)
        for j in range(1, NY):
            store_triple(s3_src, j, join(before, inside[j - 1]))
        for d in range(1, NY):
            send(s3_src.at[y_at[d]], s3_buf.at[y], s3, {"y": y_at[d]}, s3_out)
        s3_buf[y] = s3_src[y]

    def carried():
        arrived(s3_buf.at[pl.ds(0, NY - 1)], s3)
        for p in range(NY):
            state_ref[p * 32 : p * 32 + 32, :] = s3_buf[p, 0:32, :]
        return load_triple(s3_buf, 0)[1]

    enter()
    lay_weights()
    cum, lead, top_run = gates()
    end_parts()
    meet()
    send_parts()
    top_gu.z_send(0)
    low_gu.y_send()
    top_gu.y_send(0)
    top_cols = as_columns(top_run)
    loaded("q", "hg", "ng", "og", "wo", "res")
    head_gain = hg_ref[...].astype(F32).reshape(1, 256)
    feed_gain = ng_ref[...].astype(F32).reshape(1, 2048)
    for i in range(4):
        local_rows(i)
    inside = y_states()
    top_gu.z_wait(0)
    top_gu.z_send(1)
    dn.z_send(0)
    top_gu.y_send(1)
    top_gu.y_send(2)
    z_states()
    low_gu.y_forward()
    top_gu.y_forward(0)
    dn.y_send(0)
    carried_top = carried()

    def reduce_slots():
        return [slots.take(4) for _ in range(CHUNKS)]

    sums = (reduce_slots(), reduce_slots())
    gathers = [slots.take(4) for _ in range(CHUNKS)]

    def swap_send(a, i):
        send(pbuf.at[a, i, other], prcv.at[a, i], sums[a][i], to_mate, sums_out[a])

    def swap_join(a, i):
        n = sums[a][i]
        arrived(prcv.at[a, i], n)
        for j in range(NX):
            both = pbuf[a, i, c, j].astype(F32) + prcv[a, i, j].astype(F32)
            qbuf[a, i, j] = both.astype(BF16)
        top, low = pl.ds(0, half), pl.ds(half, half)
        send(qbuf.at[a, i, x_at[2], top], rly.at[a, i, 0], n + 1, to_right, sums_out[a])
        send(qbuf.at[a, i, x_at[2], low], rly.at[a, i, 1], n + 2, to_left, sums_out[a])
        if i in EARLY[a]:
            direct(a, i)

    def direct(a, i):
        n = sums[a][i]
        top, low = pl.ds(0, half), pl.ds(half, half)
        send(qbuf.at[a, i, x_at[1], low], fin.at[a, i, 0, 1], n + 3, to_right, sums_out[a])
        send(qbuf.at[a, i, x_at[3], top], fin.at[a, i, 1, 0], n + 3, to_left, sums_out[a])

    def relay(a, i):
        n = sums[a][i]
        arrived(rly.at[a, i, 0], n + 1)
        added = rly[a, i, 0].astype(F32) + qbuf[a, i, x_at[1], 0:half].astype(F32)
        rsum[a, i, 0] = added.astype(BF16)
        send(rsum.at[a, i, 0], fin.at[a, i, 0, 0], n + 3, to_right, sums_out[a])
        arrived(rly.at[a, i, 1], n + 2)
        added = rly[a, i, 1].astype(F32) + qbuf[a, i, x_at[3], half:].astype(F32)
        rsum[a, i, 1] = added.astype(BF16)
        send(rsum.at[a, i, 1], fin.at[a, i, 1, 1], n + 3, to_left, sums_out[a])
        if i not in EARLY[a]:
            direct(a, i)

    def total(a, i):
        n = sums[a][i]
        arrived(fin.at[a, i], n + 3)
        found = []
        for h in range(2):
            own = qbuf[a, i, x, h * half : h * half + half].astype(F32)
            found.append(own + fin[a, i, 0, h].astype(F32) + fin[a, i, 1, h].astype(F32))
        return jnp.concatenate(found, axis=0)

    def gated_block(g):
        part = pl.ds(g * BLOCK, BLOCK)
        run = top_cols[g * BLOCK : g * BLOCK + BLOCK]
        top = jnp.maximum(run, carried_top)
        keep = wide(jnp.exp(run - top), 2)
        enter = wide(jnp.exp(carried_top - top) * (128.0**-0.5), 2)
        earlier = jnp.dot(q_ref[part], state_ref[...], preferred_element_type=F32)
        memory = keep * num_ref[part] + enter * earlier
        mean = jnp.mean(memory * memory, axis=1, keepdims=True)
        opened = jax.nn.sigmoid(og_ref[part].astype(F32))
        gated = memory * lax.rsqrt(mean + EPSILON) * head_gain * opened
        gated = gated.astype(BF16)
        def term(j, core):
            columns = pl.ds(pl.multiple_of((2 * j + core) * 256, 256), 256)
            return jnp.dot(gated, wo_ref[:, columns], preferred_element_type=F32)

        place(0, g, term)

    def place(a, g, term):
        for core in (other, c):
            for j in range(NX):
                found = term(j, core).astype(BF16)
                for i in range(PER_BLOCK):
                    pbuf[a, g * PER_BLOCK + i, core, j] = found[i * chunk : i * chunk + chunk]
            if core is other:
                for i in range(PER_BLOCK):
                    swap_send(a, g * PER_BLOCK + i)

    def stream_chunk(i):
        n = gathers[i]
        summed = total(0, i) + res_ref[pl.ds(i * chunk, chunk)].astype(F32)
        sbuf[i, c, x] = summed.astype(BF16)
        at = sbuf.at[i, c, x]
        send(at, at, n, to_right, gather_out)
        send(at, at, n + 1, to_left, gather_out)
        send(at, at, n + 3, to_mate, gather_out)

    def spread_chunk(i):
        n = gathers[i]
        for number, d, first, device in ((n, 3, 0, to_right), (n + 1, 1, half, to_left)):
            at = sbuf.at[i, c, x_at[d]]
            arrived(at, number)
            part = sbuf.at[i, c, x_at[d], pl.ds(first, half)]
            send(part, part, n + 2, device, gather_out)
            send(at, at, n + 3, to_mate, gather_out)

    def far_chunk(i):
        n = gathers[i]
        at = sbuf.at[i, c, x_at[2]]
        arrived(at, n + 2)
        send(at, at, n + 3, to_mate, gather_out)

    def normed_chunk(i):
        arrived(sbuf.at[i, other], gathers[i] + 3)
        square = jnp.zeros((chunk, 256), F32)
        for b in range(2 * NX):
            part = sbuf[i, b % 2, b // 2].astype(F32)
            square = square + part * part
        mean = jnp.sum(square, axis=1, keepdims=True) * (1.0 / (2 * NX * 256))
        scale = lax.rsqrt(mean + EPSILON)
        for b in range(2 * NX):
            cols = slice(b * 256, b * 256 + 256)
            part = sbuf[i, b % 2, b // 2].astype(F32)
            nbuf[pl.ds(i * chunk, chunk), cols] = (part * scale * feed_gain[:, cols]).astype(BF16)

    def pump(tick):
        if tick == 0:
            top_gu.z_wait(1)
            top_gu.z_send(2)
            low_gu.y_wait()
            low_gu.z_send(0, 0)
            top_gu.y_send(3)
            top_gu.y_send(4)
            dn.z_wait(0)
            dn.z_send(1)
            dn.y_send(1)
        elif tick == 1:
            low_gu.z_send(0, 1)
        elif tick == 2:
            top_gu.y_forward(1)
            dn.y_send(2)
        elif tick == 3:
            top_gu.z_wait(2)
            top_gu.z_send(3)
            top_gu.y_send(5)
            top_gu.y_send(6)
            top_gu.y_forward(2)
        elif tick == 4:
            dn.z_wait(1)
            dn.z_send(2)
            top_gu.y_forward(3)
            dn.y_send(3)
            low_gu.z_wait(0, 0)
            low_gu.z_send(1, 0)
        elif tick == 5:
            top_gu.z_wait(3)
            top_gu.y_send(7)
            top_gu.y_forward(4)
            dn.y_send(4)
            low_gu.z_wait(0, 1)
            low_gu.z_send(1, 1)
        elif tick == 6:
            dn.z_wait(2)
            dn.z_send(3)
            top_gu.y_forward(5)
            top_gu.y_forward(6)
            dn.y_forward(0)
            dn.y_send(5)
            low_gu.z_wait(1, 0)
            low_gu.z_send(2, 0)
        elif tick == 7:
            top_gu.y_forward(7)
            dn.y_send(6)
            dn.y_forward(1)
            dn.y_forward(2)
            low_gu.z_wait(1, 1)
            low_gu.z_send(2, 1)
        elif tick == 8:
            dn.z_wait(3)
            dn.y_send(7)
            dn.y_forward(3)
            low_gu.z_wait(2, 0)
            low_gu.z_send(3, 0)
        elif tick == 9:
            dn.y_forward(4)
            dn.y_forward(5)
        elif tick == 10:
            dn.y_forward(6)
            dn.y_forward(7)
            gu_wait()
            up_block(0)
        elif tick == 11:
            up_block(1)
        elif tick == 12:
            dn_wait()
            down_block(0)

    def gu_wait():
        low_gu.taken(4, low_gu.along_z + 6)
        top_gu.y_wait()

    def dn_wait():
        dn.y_wait()

    def run(stages, pump=None):
        for tick in range(CHUNKS + max(lag for lag, _ in stages)):
            for lag, stage in stages:
                if 0 <= tick - lag < CHUNKS:
                    stage(tick - lag)
                if tick == 9 and lag == 3:
                    low_gu.z_wait(2, 1)
                    low_gu.z_send(3, 1)
            if pump is not None:
                pump(tick)

    def join_first(i):
        swap_join(0, i)

    def relay_first(i):
        relay(0, i)

    def some_gated(i):
        if i < BLOCKS:
            gated_block(i)

    def silu(v):
        return v / (1.0 + jnp.exp(-v))

    def up_block(g):
        lines = nbuf[pl.ds(g * BLOCK, BLOCK)]
        part = pl.ds(g * BLOCK, BLOCK)

        def up_cols(col, width):
            weights = gu_all[:, :, col : col + width].reshape(NZ * NY * 64, width)
            return jnp.dot(lines, weights, preferred_element_type=F32)

        for col in (0, 256):
            hidden = silu(up_cols(col, 256)) * up_cols(768 + col, 256)
            hbuf[part, col : col + 256] = hidden.astype(BF16)
        tail = up_cols(512, 256)
        hidden = silu(tail[:, :128]) * up_cols(1280, 128)
        hbuf[part, 512:640] = hidden.astype(BF16)
        mixed_tile = tail[:, 128:]
        hidden = silu(mixed_tile) * pltpu.roll(mixed_tile, 64, 1)
        lane = lax.broadcasted_iota(jnp.int32, hidden.shape, 1)
        hbuf[part, 640:768] = jnp.where(lane < 64, hidden, 0.0).astype(BF16)

    def down_block(g):
        def term(j, core):
            weights = dn_all[pl.ds((2 * j + core) * 4, 4)].reshape(256, dn_all.shape[2])
            return lax.dot_general(
                hbuf[pl.ds(g * BLOCK, BLOCK)], weights, (((1,), (1,)), ((), ())),
                preferred_element_type=F32,
            )

        place(1, g, term)

    def mixed_chunk(i):
        summed = sbuf[i, c, x].astype(F32) + 0.5 * total(1, i)
        part = pl.ds(i * chunk, chunk)
        out_ref[part] = summed.astype(BF16)
        stores.append(pltpu.make_async_copy(out_ref.at[part], out_hbm.at[part], osem.at[i]))
        stores[-1].start()

    run(
        (
            (0, some_gated), (1, join_first), (2, relay_first),
            (3, stream_chunk), (4, spread_chunk), (5, far_chunk), (6, normed_chunk),
        ),
        pump,
    )

    def drain():
        left(sbuf.at[pl.ds(0, 7)], sums_out[0])
        left(sbuf.at[pl.ds(0, 7)], gather_out)
        left(gu_all.at[pl.ds(0, 31), pl.ds(0, gu_rows)], gu_out)
        left(gu_all.at[pl.ds(0, 31), pl.ds(0, gu_rows)], low_out)
        left(dn_all.at[pl.ds(0, 31)], dn_out)
        left(s1_buf.at[pl.ds(0, NY - 1)], s1_out)
        left(s3_buf.at[pl.ds(0, NY - 1)], s3_out)
        for d in range(1, NZ):

            @pl.when(z + d < NZ)
            def _(d=d):
                state_copy(d).wait_send()

    def last(*steps):
        for name, at in steps:
            if name == "up":
                up_block(at)
            elif name == "down":
                down_block(at)
            elif name == "join":
                swap_join(1, at)
            elif name == "relay":
                relay(1, at)
            else:
                mixed_chunk(at)

    last(
        ("join", 0), ("down", 1), ("join", 1), ("up", 2), ("relay", 0), ("join", 2),
        ("relay", 1), ("down", 2), ("join", 3), ("up", 3), ("relay", 2), ("join", 4),
        ("mixed", 0), ("down", 3), ("join", 5), ("relay", 3), ("mixed", 1), ("join", 6),
        ("relay", 4), ("mixed", 2), ("join", 7), ("relay", 5), ("mixed", 3), ("relay", 6),
        ("mixed", 4), ("relay", 7), ("mixed", 5), ("mixed", 6),
    )
    drain()
    mixed_chunk(7)
    for copy in stores:
        copy.wait()
    left(sbuf.at[pl.ds(0, 7)], sums_out[1])
    assert slots.used <= RECEIVES, slots.used


RECEIVES, SENDS = 140, 15


def local(
    queries,
    cell_key_rows,
    cell_value_rows,
    output_gate_logits,
    input_gate_logits,
    forget_gate_logits,
    forget_extra_term,
    residual,
    head_norm_gain,
    cell_output_weight,
    feedforward_norm_gain,
    gate_projection_weight,
    up_projection_weight,
    down_projection_weight,
):
    rows = queries.shape[0]
    chunk = rows // CHUNKS
    half = chunk // 2
    vmem = pltpu.VMEM
    arguments = (
        queries,
        cell_key_rows,
        cell_value_rows,
        output_gate_logits,
        input_gate_logits,
        forget_gate_logits,
        forget_extra_term,
        residual,
        head_norm_gain,
        cell_output_weight,
        feedforward_norm_gain,
        gate_projection_weight,
        up_projection_weight,
        down_projection_weight.T,
    )
    scratch = [vmem(a.shape, a.dtype) for a in arguments] + [
        vmem(residual.shape, BF16),
        vmem((NZ * NY, 64, 1408), BF16),
        vmem((NZ * NY, 64, 768), BF16),
        vmem((NY, 48, 256), BF16),
        vmem((NY, 48, 256), BF16),
        vmem((1, 48, 256), BF16),
        vmem((NZ, 48, 256), BF16),
        vmem((NY, 48, 256), BF16),
        vmem((NY, 48, 256), BF16),
        vmem((128, 256), BF16),
        vmem((rows, 256), F32),
        vmem((2, CHUNKS, 2, NX, chunk, 256), BF16),
        vmem((2, CHUNKS, NX, chunk, 256), BF16),
        vmem((2, CHUNKS, NX, chunk, 256), BF16),
        vmem((2, CHUNKS, 2, half, 256), BF16),
        vmem((2, CHUNKS, 2, half, 256), BF16),
        vmem((2, CHUNKS, 2, 2, half, 256), BF16),
        vmem((CHUNKS, 2, NX, chunk, 256), BF16),
        vmem((rows, 2048), BF16),
        vmem((rows, 768), BF16),
        pltpu.SemaphoreType.DMA((SENDS,)),
        pltpu.SemaphoreType.DMA((RECEIVES,)),
        pltpu.SemaphoreType.DMA((len(arguments),)),
        pltpu.SemaphoreType.DMA((CHUNKS,)),
    ]
    return pl.pallas_call(
        cell_kernel,
        out_shape=jax.ShapeDtypeStruct(residual.shape, BF16),
        in_specs=[pl.BlockSpec(memory_space=pl.ANY)] * 14,
        out_specs=pl.BlockSpec(memory_space=pl.ANY),
        scratch_shapes=scratch,
        compiler_params=pltpu.CompilerParams(
            collective_id=0, has_side_effects=True, vmem_limit_bytes=62 * 1024 * 1024
        ),
    )(*arguments)


def solution(mesh):
    torus = Mesh(mesh.devices.reshape(NZ, NY, NX, 2), ("z", "y", "x", "c"))
    seq, head = ("z", "y"), ("x", "c")
    in_specs = (
        P(seq, head),
        P(seq, head),
        P(seq, head),
        P(seq, head),
        P(head, seq),
        P(head, seq),
        P(head, seq),
        P(seq, head),
        P(head),
        P(head, None),
        P(),
        P(seq, head),
        P(seq, head),
        P(head, seq),
    )
    return jax.shard_map(
        local, mesh=torus, in_specs=in_specs, out_specs=P(seq, head), check_vma=False
    )
```
